32 devices in a mesh: fs: 8 (over z, y), tp: 4 (over x, core).
Axes of the slice: x: 2, y: 2, z: 4, core: 2. Of those that a mesh axis runs over, the one named last changes fastest.
Arguments:
- latent_in: bfloat16 [24576, 512], P('fs'), may hold values from -6 to 6
- query_cot: bfloat16 [24576, 1536], P('fs', 'tp'), may hold values from -6 to 6
- attn_out: bfloat16 [24576, 1024], P('fs'), may hold values from -6 to 6
- mix_cot: bfloat16 [24576, 2048], P('fs', 'tp'), may hold values from -6 to 6
- query_weight: float32 [512, 1536], P('fs', 'tp'), may hold values from -0.25 to 0.25
- output_weight: float32 [1024, 2048], P('fs', 'tp'), may hold values from -0.1875 to 0.1875
- query_factor: bfloat16 [512, 256], P('fs'), may hold values from -0.25 to 0.25
- output_factor: bfloat16 [1024, 256], P('fs'), may hold values from -0.1875 to 0.1875
- query_mean: float32 [256, 1536], P('fs', 'tp'), may hold values from -3 to 3
- query_square: float32 [256, 1536], P('fs', 'tp'), may hold values from 0.05 to 1
- output_mean: float32 [256, 2048], P('fs', 'tp'), may hold values from -3 to 3
- output_square: float32 [256, 2048], P('fs', 'tp'), may hold values from 0.05 to 1
Outputs:
- step_query: float32 [512, 1536], P('fs', 'tp')
- step_output: float32 [1024, 2048], P('fs', 'tp')
- new_query: float32 [512, 1536], P('fs', 'tp')
- new_output: float32 [1024, 2048], P('fs', 'tp')
- copy_query: bfloat16 [512, 1536], P(None, 'tp')
- copy_output: bfloat16 [1024, 2048], P(None, 'tp')
- query_mean_new: float32 [256, 1536], P('fs', 'tp')
- query_square_new: float32 [256, 1536], P('fs', 'tp')
- output_mean_new: float32 [256, 2048], P('fs', 'tp')
- output_square_new: float32 [256, 2048], P('fs', 'tp')
The draws below stay inside these ranges and needn't reach their ends.
All inputs are finite; a program needn't handle non-finite values.
Results may differ from the reference program's by a relative error of at most 0.0085.
Values may be sent and summed in bfloat16 or wider, within the bound.
A program may use at most 64 MiB of HBM per device.

```python
import math
import jax
import jax.numpy as jnp
from jax import lax

D = 2048
Q_RANK = 512
RANK = 256
QCOLS = 1536
HV = 1024
TOKENS = 24576


def level_of(key, extent, cuts, smallest, top_value):
    loudness, own = 1.0, jax.random.fold_in(key, 6)
    for axis_at, blocks in cuts:
        draws = jnp.exp(jax.random.uniform(jax.random.fold_in(own, axis_at), (blocks,), jnp.float32, smallest / len(cuts), top_value / len(cuts)))
        loudness = loudness * jnp.repeat(draws, extent[axis_at] // blocks).reshape([-1 if axis == axis_at else 1 for axis in range(len(extent))])
    return loudness


def normal_values(rng, extent, width, limit, shards=(), held_as=jnp.bfloat16):
    factor_of = level_of(rng, extent, shards, -0.22, 0.18) if shards else 1.0
    values = jax.random.normal(rng, extent, jnp.float32) * width * factor_of
    return jnp.minimum(jnp.maximum(values, -limit), limit).astype(held_as)


def setup_inputs(seed: int = 0) -> dict:
    key_of = jax.random.split(jax.random.key(seed), 13)
    latent_in = normal_values(key_of[0], (TOKENS, Q_RANK), 1.0, 6.0, ((0, 8),))
    query_cot = normal_values(key_of[1], (TOKENS, QCOLS), 1.0, 6.0, ((0, 8), (1, 4)))
    attn_out = normal_values(key_of[2], (TOKENS, HV), 1.0, 6.0, ((0, 8),))
    mix_cot = normal_values(key_of[3], (TOKENS, D), 1.0, 6.0, ((0, 8), (1, 4)))
    query_weight = normal_values(key_of[4], (Q_RANK, QCOLS), Q_RANK ** -0.5, 0.25, ((0, 8), (1, 4)), jnp.float32)
    output_weight = normal_values(key_of[5], (HV, D), HV ** -0.5, 0.1875, ((0, 8), (1, 4)), jnp.float32)
    query_factor = normal_values(key_of[6], (Q_RANK, RANK), Q_RANK ** -0.5, 0.25, ((0, 8),))
    output_factor = normal_values(key_of[7], (HV, RANK), HV ** -0.5, 0.1875, ((0, 8),))
    query_mean = normal_values(key_of[8], (RANK, QCOLS), 0.5, 3.0, ((0, 8), (1, 4)), jnp.float32)
    query_square = jnp.clip(jnp.exp(math.log(1.0) - 2.9957323 * jax.random.uniform(key_of[9], (RANK, QCOLS), jnp.float32) ** level_of(key_of[9], (RANK, QCOLS), ((0, 8), (1, 4)), -0.2, 0.2)), 0.05, 1.0)
    output_mean = normal_values(key_of[10], (RANK, D), 0.5, 3.0, ((0, 8), (1, 4)), jnp.float32)
    output_square = jnp.clip(jnp.exp(math.log(1.0) - 2.9957323 * jax.random.uniform(key_of[11], (RANK, D), jnp.float32) ** level_of(key_of[11], (RANK, D), ((0, 8), (1, 4)), -0.2, 0.2)), 0.05, 1.0)
    return {"latent_in": latent_in, "query_cot": query_cot, "attn_out": attn_out, "mix_cot": mix_cot, "query_weight": query_weight, "output_weight": output_weight, "query_factor": query_factor, "output_factor": output_factor, "query_mean": query_mean, "query_square": query_square, "output_mean": output_mean, "output_square": output_square}


def over_rows(left, right):
    return lax.dot_general(left, right, (((0,), (0,)), ((), ())), preferred_element_type=jnp.float32)

def exact_dot(left, right):
    return jnp.dot(left, right, precision=lax.Precision.HIGHEST, preferred_element_type=jnp.float32)

def moments(mean, square, low):
    mean_new = 0.8 * mean + 0.2 * low
    square_new = 0.9 * square + 0.1 * low * low
    return (mean_new, square_new, mean_new / jnp.sqrt(square_new))

def reference(latent_in, query_cot, attn_out, mix_cot, query_weight, output_weight, query_factor, output_factor, query_mean, query_square, output_mean, output_square):
    inv_root = 1.0 / math.sqrt(latent_in.shape[0])
    grad_query = over_rows(latent_in, query_cot) * inv_root
    grad_output = over_rows(attn_out, mix_cot) * inv_root
    factor_query = query_factor.astype(jnp.float32)
    factor_output = output_factor.astype(jnp.float32)
    low_query = exact_dot(factor_query.T, grad_query)
    low_output = exact_dot(factor_output.T, grad_output)
    mean_q, square_q, direction_q = moments(query_mean, query_square, low_query)
    mean_o, square_o, direction_o = moments(output_mean, output_square, low_output)
    scale_q = 1.0 / jnp.sqrt(jnp.mean(direction_q * direction_q) + 0.25)
    scale_o = 1.0 / jnp.sqrt(jnp.mean(direction_o * direction_o) + 0.25)
    step_q = exact_dot(factor_query, direction_q) * scale_q
    step_o = exact_dot(factor_output, direction_o) * scale_o
    new_q = query_weight - 0.02 * step_q
    new_o = output_weight - 0.02 * step_o
    return (step_q, step_o, new_q, new_o, new_q.astype(jnp.bfloat16), new_o.astype(jnp.bfloat16), mean_q, square_q, mean_o, square_o)
```

```python
import functools
import math

import jax
import jax.numpy as jnp
from jax import lax
from jax.experimental import pallas as pl
from jax.experimental.pallas import tpu as pltpu
from jax.sharding import PartitionSpec as P

MESH = pl.DeviceIdType.MESH
BF16 = jnp.bfloat16
F32 = jnp.float32
CHUNKS = 4


def grid_of(count):
    inner = max(d for d in range(1, count + 1) if count % d == 0 and d * d <= count)
    return count // inner, inner


def semaphores_of(nz, ny, nt):
    z_kinds, y_kinds = 2 + 2 + 2 + 2, 2 + 2 + 2
    return z_kinds * nz + y_kinds * nz * (ny - 1) + 2 * (ny - 1) + 4 * ny + nt + nz * ny + 4


def over_rows(left, right):
    return lax.dot_general(left, right, (((0,), (0,)), ((), ())), preferred_element_type=F32)


def exchange_kernel(
    nz, ny, nt, inv_root,
    latent_hbm, cot_hbm, attn_hbm, mix_hbm, wq_hbm, wo_hbm, fq_hbm, fo_hbm,
    qm_hbm, qs_hbm, om_hbm, os_hbm,
    fq_all, fo_all, wq_all, wo_all, dq_all, do_all, total, qm_new, qs_new, om_new, os_new,
    latent, cot, attn, mix, wq, wo, qm, qs, om, os_, grad_q, grad_o,
    part_q, part_o, yin_q, yin_o, acc_q, acc_o, zout_q, zout_o, zin_q, zin_o,
    tile_tp, tile_fs,
    load_sem, own_sem, send_sem, recv_sem,
):
    n = nz * ny
    f = lax.axis_index("fs")
    t = lax.axis_index("tp")
    z, y = f // ny, f % ny
    half_cols = fq_all.shape[-1] // 2
    half = pl.ds(pl.multiple_of((t % 2) * half_cols, half_cols), half_cols)
    twin = t + 1 - 2 * (t % 2)
    step = latent_hbm.shape[0] // CHUNKS

    barrier = pltpu.get_barrier_semaphore()
    for d in range(1, n):
        pl.semaphore_signal(barrier, inc=1, device_id={"fs": (f + d) % n}, device_id_type=MESH)
    for d in range(1, nt):
        pl.semaphore_signal(barrier, inc=1, device_id={"tp": (t + d) % nt}, device_id_type=MESH)

    own = [
        pltpu.make_async_copy(src, dst, own_sem.at[i])
        for i, (src, dst) in enumerate((
            (fo_hbm.at[:, half], fo_all.at[z, y, :, half]),
            (fq_hbm.at[:, half], fq_all.at[z, y, :, half]),
            (wo_hbm, wo), (wq_hbm, wq),
            (om_hbm, om), (os_hbm, os_), (qm_hbm, qm), (qs_hbm, qs),
        ))
    ]
    for c in own[:4]:
        c.start()

    def load(k, pair, sem):
        rows = pl.ds(pl.multiple_of(k * step, step), step)
        return [
            pltpu.make_async_copy(src.at[rows, :], dst.at[rows, :], load_sem.at[k, sem + i])
            for i, (src, dst) in enumerate(pair)
        ]

    pair_o = ((attn_hbm, attn), (mix_hbm, mix))
    pair_q = ((latent_hbm, latent), (cot_hbm, cot))
    with jax.named_scope("own"):
        for c in own[:4]:
            c.wait()
    for k in range(CHUNKS):
        for c in load(k, pair_o, 0):
            c.start()
    for k in range(CHUNKS):
        for c in load(k, pair_q, 2):
            c.start()
    for c in own[4:]:
        c.start()
    wo_all[z, y] = wo[...].astype(BF16)
    wq_all[z, y] = wq[...].astype(BF16)
    with jax.named_scope("barrier"):
        pl.semaphore_wait(barrier, n - 1 + nt - 1)

    used = [0]
    sent = []

    def room(count):
        at = used[0]
        used[0] = at + count
        return at

    def remote(src, dst, device, at, to):
        return pltpu.make_async_remote_copy(
            src_ref=src, dst_ref=dst, send_sem=send_sem.at[at], recv_sem=recv_sem.at[to],
            device_id=device, device_id_type=MESH,
        )

    def launch(c):
        c.start()
        sent.append(c)
        return c

    lower, upper = z, nz - 1 - z
    both = jnp.minimum(lower, upper)

    def near(k):
        paired = k < 2 * both
        away = jnp.where(paired, k // 2 + 1, k - both + 1)
        down = jnp.where(paired, k % 2 == 0, lower > upper)
        return jnp.where(down, z - away, z + away)

    others = [near(k) for k in range(nz - 1)]

    class Along:
        def __init__(self, block, landing=None):
            self.block, self.landing, self.at = block, landing or block, room(nz)

        def to(self, zz):
            return remote(
                self.block(z) if self.landing is self.block else self.block(zz), self.landing(z),
                {"fs": zz * ny + y}, self.at + zz, self.at + z,
            )

        def wait(self, zz):
            remote(
                self.landing(zz), self.landing(zz), {"fs": zz * ny + y}, self.at + zz, self.at + zz
            ).wait_recv()

    class Across:
        def __init__(self, block):
            self.block, self.at = block, room(nz * (ny - 1))

        def send(self, zz):
            for d in range(1, ny):
                k = self.at + (d - 1) * nz + zz
                launch(remote(
                    self.block(zz, y), self.block(zz, y), {"fs": z * ny + (y + d) % ny}, k, k
                ))

        def wait(self, zz):
            for d in range(1, ny):
                k = self.at + (d - 1) * nz + zz
                block = self.block(zz, (y + ny - d) % ny)
                remote(block, block, {"fs": z * ny + (y + d) % ny}, k, k).wait_recv()

    fo_z = Along(lambda zz: fo_all.at[zz, y, :, half])
    fq_z = Along(lambda zz: fq_all.at[zz, y, :, half])
    fo_y = Across(lambda zz, yy: fo_all.at[zz, yy, :, half])
    fq_y = Across(lambda zz, yy: fq_all.at[zz, yy, :, half])
    wo_z = Along(lambda zz: wo_all.at[zz, y])
    wq_z = Along(lambda zz: wq_all.at[zz, y])
    wo_y = Across(lambda zz, yy: wo_all.at[zz, yy])
    wq_y = Across(lambda zz, yy: wq_all.at[zz, yy])
    do_z = Along(lambda zz: do_all.at[zz, y])
    dq_z = Along(lambda zz: dq_all.at[zz, y])
    do_y = Across(lambda zz, yy: do_all.at[zz, yy])
    dq_y = Across(lambda zz, yy: dq_all.at[zz, yy])

    for fac_z, fac_y in ((fo_z, fo_y), (fq_z, fq_y)):
        for zz in others:
            launch(fac_z.to(zz))
        fac_y.send(z)

    through = nz >= 3
    inside = jnp.logical_and(z > 0, z < nz - 1)
    far = []
    for k, zz in enumerate(others):
        for w_z in (wq_z, wo_z):
            c = w_z.to(zz)
            if through and k == nz - 2:
                far.append(c)
                pl.when(inside)(c.start)
            else:
                launch(c)
    wo_y.send(z)

    def product(k, pair, sem, out):
        for c in load(k, pair, sem):
            c.wait()
        rows = pl.ds(pl.multiple_of(k * step, step), step)
        new = over_rows(pair[1][1][rows, :], pair[0][1][rows, :])
        out[...] += new

    def products(lo, hi, pair, sem, out):
        @pl.loop(lo, hi)
        def _(k):
            product(k, pair, sem, out)

    grad_o[...] = jnp.zeros_like(grad_o)
    grad_q[...] = jnp.zeros_like(grad_q)
    swaps = {}

    def swap(all_, yy):
        block = all_.at[:, yy, :, half]
        k = room(1)
        return launch(remote(block, block, {"tp": twin}, k, k))

    with jax.named_scope("prod_o"):
        products(0, CHUNKS - 1, pair_o, 0, grad_o)
    for zz in others:
        with jax.named_scope("wait_foz"):
            fo_z.wait(zz)
        fo_y.send(zz)
    swaps["o"] = [swap(fo_all, y)]
    with jax.named_scope("prod_o"):
        products(CHUNKS - 1, CHUNKS, pair_o, 0, grad_o)
    for zz in others:
        with jax.named_scope("wait_fqz"):
            fq_z.wait(zz)
        fq_y.send(zz)
    swaps["q"] = [swap(fq_all, y)]
    wq_y.send(z)
    with jax.named_scope("prod_q"):
        products(0, CHUNKS, pair_q, 2, grad_q)

    rank = fq_all.shape[-1]
    block = rank // n

    def project(factor_all, grad, part):
        factor = factor_all[...].reshape(-1, rank)
        low = lax.dot_general(
            factor, grad[...].astype(BF16), (((0,), (1,)), ((), ())), preferred_element_type=F32
        ) * inv_root
        for i in range(nz):
            for j in range(ny):
                at = (i * ny + j) * block
                part[i, j] = low[at:at + block, :]

    matrices = (
        ("o", fo_all, fo_y, grad_o, part_o, yin_o, acc_o, zout_o, zin_o),
        ("q", fq_all, fq_y, grad_q, part_q, yin_q, acc_q, zout_q, zin_q),
    )
    y_in = []
    for name, all_, fac_y, grad, part, yin, acc, zout, zin in matrices:
        with jax.named_scope("wait_fy"):
            for zz in [z] + others:
                fac_y.wait(zz)
        for d in range(1, ny):
            swaps[name].append(swap(all_, (y + ny - d) % ny))
        with jax.named_scope("wait_swap"):
            for c in swaps[name]:
                c.wait_recv()
        with jax.named_scope("project"):
            project(all_, grad, part)
        copies = []
        for d in range(1, ny):
            yy = (y + d) % ny
            for i in range(nz):
                yin[ny - 1 + d - 1, i] = part[i, yy].astype(BF16)
            k = room(1)
            copies.append(launch(remote(
                yin.at[ny - 1 + d - 1], yin.at[d - 1], {"fs": z * ny + yy}, k, k
            )))
        y_in.append(copies)

    def forward_weights(k):
        zz = others[k]
        with jax.named_scope("wait_wz"):
            wq_z.wait(zz)
            wo_z.wait(zz)
        wo_y.send(zz)
        wq_y.send(zz)

    if nz > 1:
        forward_weights(0)

    low_z = []
    for (name, _, _, _, part, yin, acc, zout, zin), copies in zip(matrices, y_in):
        for i in range(nz):
            acc[i] = part[i, y]
        for d, c in enumerate(copies):
            with jax.named_scope("wait_y"):
                c.wait_recv()
            for i in range(nz):
                acc[i] += yin[d, i].astype(F32)
        along = Along(lambda zz, zout=zout: zout.at[zz], lambda zz, zin=zin: zin.at[zz])
        for zz in others:
            zout[zz] = acc[zz].astype(BF16)
            launch(along.to(zz))
        low_z.append(along)

    if nz > 2:
        forward_weights(1)

    if through:
        ahead = []
        for edge, here in ((0, nz - 2), (nz - 1, 1)):
            for w_z in (wq_z, wo_z):
                k = room(1)
                ahead.append((here, edge, w_z, remote(
                    w_z.block(edge), w_z.block(edge), {"fs": (nz - 1 - edge) * ny + y},
                    k, w_z.at + edge,
                )))

    sides = (
        (matrices[0], low_z[0], om, os_, om_new, os_new, do_all, do_z, do_y, 1),
        (matrices[1], low_z[1], qm, qs, qm_new, qs_new, dq_all, dq_z, dq_y, 0),
    )
    for c in own[4:]:
        c.wait()
    for (_, _, _, _, _, _, acc, _, zin), along, mean, square, mean_out, square_out, d_all, d_z, d_y, slot in sides:
        low = acc[z]
        for zz in others:
            with jax.named_scope("wait_z"):
                along.wait(zz)
            low += zin[zz].astype(F32)
        mean_new = 0.8 * mean[...] + 0.2 * low
        square_new = 0.9 * square[...] + 0.1 * low * low
        mean_out[...] = mean_new
        square_out[...] = square_new
        direction = mean_new / jnp.sqrt(square_new)
        d_all[z, y] = direction.astype(BF16)
        for zz in others:
            launch(d_z.to(zz))
        d_y.send(z)
        tile_tp[0, slot] = jnp.broadcast_to(jnp.sum(direction * direction), tile_tp.shape[2:])

    tiles = []
    for d in range(1, nt):
        k = room(1)
        tiles.append(launch(remote(tile_tp.at[0], tile_tp.at[d], {"tp": (t + d) % nt}, k, k)))

    if through:
        @pl.when(inside)
        def _():
            with jax.named_scope("wait_far"):
                wq_z.wait(others[nz - 2])
                wo_z.wait(others[nz - 2])
        for here, edge, w_z, c in ahead:
            pl.when(z == here)(c.start)

    with jax.named_scope("wait_tp"):
        for c in tiles:
            c.wait_recv()
    tile_fs[0] = jnp.sum(tile_tp[...], axis=0)
    tiles = []
    for d in range(1, n):
        k = room(1)
        tiles.append(launch(remote(tile_fs.at[0], tile_fs.at[d], {"fs": (f + d) % n}, k, k)))
    for d_z, d_y in ((do_z, do_y), (dq_z, dq_y)):
        for zz in others:
            with jax.named_scope("wait_dz"):
                d_z.wait(zz)
            d_y.send(zz)

    for k in range(2, nz - 1):
        zz = others[k]
        if through and k == nz - 2:
            with jax.named_scope("wait_wz_last"):
                @pl.when(jnp.logical_not(inside))
                def _():
                    wq_z.wait(zz)
                    wo_z.wait(zz)
        else:
            wq_z.wait(zz)
            wo_z.wait(zz)
        wo_y.send(zz)
        wq_y.send(zz)

    with jax.named_scope("wait_fs"):
        for c in tiles:
            c.wait_recv()
    total[...] = jnp.sum(tile_fs[...], axis=0)
    with jax.named_scope("wait_dy"):
        for zz in [z] + others:
            do_y.wait(zz)
            dq_y.wait(zz)
    with jax.named_scope("wait_wy"):
        for zz in [z] + others:
            wo_y.wait(zz)
            wq_y.wait(zz)
    for c in sent:
        c.wait_send()
    for c in far:
        pl.when(inside)(c.wait_send)
    if through:
        for here, edge, w_z, c in ahead:
            pl.when(z == here)(c.wait_send)


def finish_kernel(
    nz, ny, nt,
    fq_all, fo_all, wq_all, wo_all, dq_all, do_all, total, wq, wo, qm, qs, om, os_,
    step_q_hbm, step_o_hbm, new_q_hbm, new_o_hbm, copy_q_hbm, copy_o_hbm,
    qm_hbm, qs_hbm, om_hbm, os_hbm,
    step_q, step_o, new_q, new_o, copy_q, copy_o,
    sem,
):
    f = lax.axis_index("fs")
    z, y = f // ny, f % ny
    started = []

    def put(src, dst):
        c = pltpu.make_async_copy(src, dst, sem.at[len(started)])
        c.start()
        started.append(c)

    for src, dst in ((qm, qm_hbm), (qs, qs_hbm), (om, om_hbm), (os_, os_hbm)):
        put(src, dst)
    rank = fq_all.shape[-1]
    for slot, f_all, w_all, d_all, w, step, new, copy, step_hbm, new_hbm, copy_hbm in (
        (1, fo_all, wo_all, do_all, wo, step_o, new_o, copy_o, step_o_hbm, new_o_hbm, copy_o_hbm),
        (0, fq_all, wq_all, dq_all, wq, step_q, new_q, copy_q, step_q_hbm, new_q_hbm, copy_q_hbm),
    ):
        cols = w.shape[1]
        scale = lax.rsqrt(total[slot] / (rank * cols * nt) + 0.25)[0:1, 0:1]
        direction = d_all[...].reshape(rank, cols)
        rows = f_all.shape[2]
        for i in range(nz):
            full = jnp.dot(
                f_all[i].reshape(ny * rows, rank), direction, preferred_element_type=F32
            ) * scale
            at = pl.ds(i * ny * rows, ny * rows)
            old = w_all[i].reshape(ny * rows, cols).astype(F32)
            copy[at, :] = (old - 0.02 * full).astype(BF16)
            put(copy.at[at, :], copy_hbm.at[at, :])
        own = jnp.dot(f_all[z, y], direction, preferred_element_type=F32) * scale
        step[...] = own
        new[...] = w[...] - 0.02 * own
        put(step, step_hbm)
        put(new, new_hbm)
    for c in started:
        c.wait()


def on_device(
    nz, ny, nt,
    latent_in, query_cot, attn_out, mix_cot, query_weight, output_weight,
    query_factor, output_factor, query_mean, query_square, output_mean, output_square,
):
    n = nz * ny
    tokens = latent_in.shape[0]
    inv_root = 1.0 / math.sqrt(tokens * n)
    rq, cq = query_weight.shape
    ro, co = output_weight.shape
    rank = query_factor.shape[1]
    block = rank // n
    vmem = pl.BlockSpec(memory_space=pltpu.VMEM)
    hbm = pl.BlockSpec(memory_space=pltpu.HBM)
    copies = semaphores_of(nz, ny, nt)
    fq, fo, wq, wo, dq, do, total, qm, qs, om, os_ = pl.pallas_call(
        functools.partial(exchange_kernel, nz, ny, nt, inv_root),
        name="moment_exchange",
        in_specs=[hbm] * 12,
        out_specs=[vmem] * 11,
        out_shape=[
            jax.ShapeDtypeStruct((nz, ny, rq, rank), BF16),
            jax.ShapeDtypeStruct((nz, ny, ro, rank), BF16),
            jax.ShapeDtypeStruct((nz, ny, rq, cq), BF16),
            jax.ShapeDtypeStruct((nz, ny, ro, co), BF16),
            jax.ShapeDtypeStruct((nz, ny, block, cq), BF16),
            jax.ShapeDtypeStruct((nz, ny, block, co), BF16),
            jax.ShapeDtypeStruct((2, 8, 128), F32),
            jax.ShapeDtypeStruct((block, cq), F32),
            jax.ShapeDtypeStruct((block, cq), F32),
            jax.ShapeDtypeStruct((block, co), F32),
            jax.ShapeDtypeStruct((block, co), F32),
        ],
        scratch_shapes=[
            pltpu.VMEM(latent_in.shape, BF16),
            pltpu.VMEM(query_cot.shape, BF16),
            pltpu.VMEM(attn_out.shape, BF16),
            pltpu.VMEM(mix_cot.shape, BF16),
            pltpu.VMEM((rq, cq), F32),
            pltpu.VMEM((ro, co), F32),
            pltpu.VMEM((block, cq), F32),
            pltpu.VMEM((block, cq), F32),
            pltpu.VMEM((block, co), F32),
            pltpu.VMEM((block, co), F32),
            pltpu.VMEM((cq, n * rq), F32),
            pltpu.VMEM((co, n * ro), F32),
            pltpu.VMEM((nz, ny, block, cq), F32),
            pltpu.VMEM((nz, ny, block, co), F32),
            pltpu.VMEM((2 * max(ny - 1, 1), nz, block, cq), BF16),
            pltpu.VMEM((2 * max(ny - 1, 1), nz, block, co), BF16),
            pltpu.VMEM((nz, block, cq), F32),
            pltpu.VMEM((nz, block, co), F32),
            pltpu.VMEM((nz, block, cq), BF16),
            pltpu.VMEM((nz, block, co), BF16),
            pltpu.VMEM((nz, block, cq), BF16),
            pltpu.VMEM((nz, block, co), BF16),
            pltpu.VMEM((nt, 2, 8, 128), F32),
            pltpu.VMEM((n, 2, 8, 128), F32),
            pltpu.SemaphoreType.DMA((CHUNKS, 4)),
            pltpu.SemaphoreType.DMA((8,)),
            pltpu.SemaphoreType.DMA((copies,)),
            pltpu.SemaphoreType.DMA((copies,)),
        ],
        compiler_params=pltpu.CompilerParams(
            collective_id=0, has_side_effects=True, vmem_limit_bytes=40 * 1024 * 1024
        ),
    )(*(pltpu.with_memory_space_constraint(a, pltpu.HBM) for a in (
        latent_in, query_cot, attn_out, mix_cot, query_weight, output_weight,
        query_factor, output_factor, query_mean, query_square, output_mean, output_square,
    )))
    shapes = (
        ((rq, cq), F32), ((ro, co), F32), ((rq, cq), F32), ((ro, co), F32),
        ((n * rq, cq), BF16), ((n * ro, co), BF16),
        ((block, cq), F32), ((block, cq), F32), ((block, co), F32), ((block, co), F32),
    )
    return pl.pallas_call(
        functools.partial(finish_kernel, nz, ny, nt),
        name="finish",
        in_specs=[vmem] * 13,
        out_specs=[hbm] * 10,
        out_shape=[jax.ShapeDtypeStruct(*s) for s in shapes],
        scratch_shapes=[pltpu.VMEM(*s) for s in shapes[:6]]
        + [pltpu.SemaphoreType.DMA((2 * nz + 8,))],
        compiler_params=pltpu.CompilerParams(vmem_limit_bytes=20 * 1024 * 1024),
    )(fq, fo, wq, wo, dq, do, total, query_weight, output_weight, qm, qs, om, os_)


def solution(mesh):
    nz, ny = grid_of(mesh.shape["fs"])
    rows, both, cols = P("fs", None), P("fs", "tp"), P(None, "tp")
    return jax.shard_map(
        functools.partial(on_device, nz, ny, mesh.shape["tp"]),
        mesh=mesh,
        in_specs=(rows, both, rows, both, both, both, rows, rows, both, both, both, both),
        out_specs=(both, both, both, both, cols, cols, both, both, both, both),
        check_vma=False,
    )
```

```python
import functools
import math

import jax
import jax.numpy as jnp
from jax import lax
from jax.experimental import pallas as pl
from jax.experimental.pallas import tpu as pltpu
from jax.sharding import PartitionSpec as P

MESH = pl.DeviceIdType.MESH
BF16 = jnp.bfloat16
F32 = jnp.float32
CHUNKS = 4


def grid_of(count):
    inner = max(d for d in range(1, count + 1) if count % d == 0 and d * d <= count)
    return count // inner, inner


def semaphores_of(nz, ny, nt):
    z_kinds, y_kinds = 2 + 2 + 2 + 2, 2 + 2 + 2
    return z_kinds * nz + y_kinds * nz * (ny - 1) + 6 * (ny - 1) + 2 * ny + nt + nz * ny + 4


def over_rows(left, right):
    return lax.dot_general(left, right, (((0,), (0,)), ((), ())), preferred_element_type=F32)


def exchange_kernel(
    nz, ny, nt, inv_root,
    latent_hbm, cot_hbm, attn_hbm, mix_hbm, wq_hbm, wo_hbm, fq_hbm, fo_hbm,
    qm_hbm, qs_hbm, om_hbm, os_hbm,
    fq_all, fo_all, wq_all, wo_all, dq_all, do_all, total, qm_new, qs_new, om_new, os_new,
    latent, cot, attn, mix, wq, wo, qm, qs, om, os_, grad_q, grad_o,
    part_q, part_o, yin_q, yin_o, acc_q, acc_o, zout_q, zout_o, zin_q, zin_o,
    tile_tp, tile_fs, rounded_q, rounded_o,
    load_sem, own_sem, send_sem, recv_sem,
):
    n = nz * ny
    f = lax.axis_index("fs")
    t = lax.axis_index("tp")
    z, y = f // ny, f % ny
    half_cols = fq_all.shape[-1]
    core = t % 2
    half = pl.ds(pl.multiple_of(core * half_cols, half_cols), half_cols)
    twin = t + 1 - 2 * (t % 2)
    step = latent_hbm.shape[0] // CHUNKS

    barrier = pltpu.get_barrier_semaphore()
    for d in range(1, n):
        pl.semaphore_signal(barrier, inc=1, device_id={"fs": (f + d) % n}, device_id_type=MESH)
    for d in range(1, nt):
        pl.semaphore_signal(barrier, inc=1, device_id={"tp": (t + d) % nt}, device_id_type=MESH)

    own = [
        pltpu.make_async_copy(src, dst, own_sem.at[i])
        for i, (src, dst) in enumerate((
            (fo_hbm.at[:, half], fo_all.at[core, z, y]),
            (fq_hbm.at[:, half], fq_all.at[core, z, y]),
            (wo_hbm, wo), (wq_hbm, wq),
            (om_hbm, om), (os_hbm, os_), (qm_hbm, qm), (qs_hbm, qs),
        ))
    ]
    for c in own[:4]:
        c.start()

    def load(k, pair, sem):
        rows = pl.ds(pl.multiple_of(k * step, step), step)
        return [
            pltpu.make_async_copy(src.at[rows, :], dst.at[rows, :], load_sem.at[k, sem + i])
            for i, (src, dst) in enumerate(pair)
        ]

    pair_o = ((attn_hbm, attn), (mix_hbm, mix))
    pair_q = ((latent_hbm, latent), (cot_hbm, cot))
    with jax.named_scope("own"):
        for c in own[:4]:
            c.wait()
    for k in range(CHUNKS):
        for c in load(k, pair_o, 0):
            c.start()
    for k in range(CHUNKS):
        for c in load(k, pair_q, 2):
            c.start()
    for c in own[4:]:
        c.start()
    wo_all[z, y] = wo[...].astype(BF16)
    wq_all[z, y] = wq[...].astype(BF16)
    with jax.named_scope("barrier"):
        pl.semaphore_wait(barrier, n - 1 + nt - 1)

    used = [0]
    sent = []

    def room(count):
        at = used[0]
        used[0] = at + count
        return at

    def remote(src, dst, device, at, to):
        return pltpu.make_async_remote_copy(
            src_ref=src, dst_ref=dst, send_sem=send_sem.at[at], recv_sem=recv_sem.at[to],
            device_id=device, device_id_type=MESH,
        )

    def launch(c):
        c.start()
        sent.append(c)
        return c

    lower, upper = z, nz - 1 - z
    both = jnp.minimum(lower, upper)

    def near(k):
        paired = k < 2 * both
        away = jnp.where(paired, k // 2 + 1, k - both + 1)
        down = jnp.where(paired, (k + z) % 2 == 1, lower > upper)
        return jnp.where(down, z - away, z + away)

    others = [near(k) for k in range(nz - 1)]

    class Along:
        def __init__(self, block, landing=None):
            self.block, self.landing, self.at = block, landing or block, room(nz)

        def to(self, zz):
            return remote(
                self.block(z) if self.landing is self.block else self.block(zz), self.landing(z),
                {"fs": zz * ny + y}, self.at + zz, self.at + z,
            )

        def wait(self, zz):
            remote(
                self.landing(zz), self.landing(zz), {"fs": zz * ny + y}, self.at + zz, self.at + zz
            ).wait_recv()

    class Across:
        def __init__(self, block):
            self.block, self.at = block, room(nz * (ny - 1))

        def copies(self, zz):
            ks = [self.at + (d - 1) * nz + zz for d in range(1, ny)]
            return [
                remote(self.block(zz, y), self.block(zz, y), {"fs": z * ny + (y + d) % ny}, k, k)
                for d, k in zip(range(1, ny), ks)
            ]

        def send(self, zz):
            for c in self.copies(zz):
                launch(c)

        def wait(self, zz):
            for d in range(1, ny):
                k = self.at + (d - 1) * nz + zz
                block = self.block(zz, (y + ny - d) % ny)
                remote(block, block, {"fs": z * ny + (y + d) % ny}, k, k).wait_recv()

    fo_z = Along(lambda zz: fo_all.at[core, zz, y])
    fq_z = Along(lambda zz: fq_all.at[core, zz, y])
    fo_y = Across(lambda zz, yy: fo_all.at[core, zz, yy])
    fq_y = Across(lambda zz, yy: fq_all.at[core, zz, yy])
    wo_z = Along(lambda zz: wo_all.at[zz, y])
    wq_z = Along(lambda zz: wq_all.at[zz, y])
    wo_y = Across(lambda zz, yy: wo_all.at[zz, yy])
    wq_y = Across(lambda zz, yy: wq_all.at[zz, yy])
    do_z = Along(lambda zz: do_all.at[zz, y])
    dq_z = Along(lambda zz: dq_all.at[zz, y])
    do_y = Across(lambda zz, yy: do_all.at[zz, yy])
    dq_y = Across(lambda zz, yy: dq_all.at[zz, yy])

    for fac_z, fac_y in ((fo_z, fo_y), (fq_z, fq_y)):
        for zz in others:
            launch(fac_z.to(zz))
        fac_y.send(z)
    wo_y.send(z)

    through = nz >= 3
    mated = nz % 2 == 0
    inside = jnp.logical_and(z > 0, z < nz - 1)
    far = []

    def send_weights(w_z, ks):
        for k in ks:
            c = w_z.to(others[k])
            if through and k == nz - 2:
                far.append(c)
                pl.when(inside)(c.start)
            else:
                launch(c)

    outward = list(reversed(range(nz - 1)))

    def product(k, pair, sem, out):
        for c in load(k, pair, sem):
            c.wait()
        rows = pl.ds(pl.multiple_of(k * step, step), step)
        new = over_rows(pair[1][1][rows, :], pair[0][1][rows, :])
        out[...] += new

    def products(lo, hi, pair, sem, out):
        @pl.loop(lo, hi)
        def _(k):
            product(k, pair, sem, out)

    grad_o[...] = jnp.zeros_like(grad_o)
    grad_q[...] = jnp.zeros_like(grad_q)
    swaps = {}

    def swap(all_, yy):
        block = all_.at[core, :, yy]
        k = room(1)
        return launch(remote(block, block, {"tp": twin}, k, k))

    early = CHUNKS // 2
    with jax.named_scope("prod_o"):
        products(0, early, pair_o, 0, grad_o)
    for k, zz in enumerate(others):
        with jax.named_scope("wait_foz"):
            fo_z.wait(zz)
        fo_y.send(zz)
        if k == min(1, nz - 2):
            send_weights(wo_z, outward)
            send_weights(wq_z, [0])
        if early < CHUNKS:
            with jax.named_scope("prod_o"):
                products(early, early + 1, pair_o, 0, grad_o)
            early += 1
    swaps["o"] = [swap(fo_all, y)]
    with jax.named_scope("prod_o"):
        if early < CHUNKS:
            products(early, CHUNKS, pair_o, 0, grad_o)
    for zz in others:
        with jax.named_scope("wait_fqz"):
            fq_z.wait(zz)
        fq_y.send(zz)
    swaps["q"] = [swap(fq_all, y)]
    wq_y.send(z)
    with jax.named_scope("prod_q"):
        products(0, CHUNKS, pair_q, 2, grad_q)

    rank = 2 * half_cols
    block = rank // n
    per_half = nz // 2

    def project(h, factor_all, grad, part):
        factor = factor_all[h].reshape(-1, half_cols)
        low = lax.dot_general(
            factor, grad[...], (((0,), (1,)), ((), ())), preferred_element_type=F32
        ) * inv_root
        for i in range(per_half):
            for j in range(ny):
                at = (i * ny + j) * block
                part[h * per_half + i, j] = low[at:at + block, :]

    matrices = (
        ("o", fo_all, fo_y, grad_o, rounded_o, part_o, yin_o, acc_o, zout_o, zin_o),
        ("q", fq_all, fq_y, grad_q, rounded_q, part_q, yin_q, acc_q, zout_q, zin_q),
    )
    units = []
    for name, all_, fac_y, grad, rounded, part, yin, acc, zout, zin in matrices:
        rounded[...] = grad[...].astype(BF16)
        along = Along(lambda zz, zout=zout: zout.at[zz], lambda zz, zin=zin: zin.at[zz])
        with jax.named_scope("wait_fy"):
            for zz in [z] + others:
                fac_y.wait(zz)
        for d in range(1, ny):
            swaps[name].append(swap(all_, (y + ny - d) % ny))
        for turn, h in enumerate((core, 1 - core)):
            if turn:
                with jax.named_scope("wait_swap"):
                    for c in swaps[name]:
                        c.wait_recv()
            with jax.named_scope("project"):
                project(h, all_, rounded, part)
            rows = pl.ds(h * per_half, per_half)
            copies = []
            for d in range(1, ny):
                yy = (y + d) % ny
                for i in range(per_half):
                    yin[ny - 1 + d - 1, h * per_half + i] = part[h * per_half + i, yy].astype(BF16)
                k = room(1)
                copies.append(launch(remote(
                    yin.at[ny - 1 + d - 1, rows], yin.at[d - 1, rows], {"fs": z * ny + yy}, k, k
                )))
            units.append((h, part, yin, acc, zout, along, copies))

    def forward(k, w_z, w_y):
        with jax.named_scope("wait_wz"):
            w_z.wait(others[k])
        w_y.send(others[k])

    if nz > 1 and not mated:
        forward(0, wo_z, wo_y)
        forward(0, wq_z, wq_y)

    ahead = []

    def relay(w_z):
        if not through:
            return
        mine = []
        for edge, here in ((0, nz - 2), (nz - 1, 1)):
            k = room(1)
            mine.append((here, remote(
                w_z.block(edge), w_z.block(edge), {"fs": (nz - 1 - edge) * ny + y},
                k, w_z.at + edge,
            )))

        @pl.when(inside)
        def _():
            with jax.named_scope("wait_far"):
                w_z.wait(others[nz - 2])
        for here, c in mine:
            pl.when(z == here)(c.start)
        ahead.extend(mine)

    def forward_far(w_z, w_y, at_edge):
        if not through:
            return
        if at_edge:
            @pl.when(jnp.logical_not(inside))
            def _():
                with jax.named_scope("wait_wz_last"):
                    w_z.wait(others[nz - 2])
        cs = w_y.copies(others[nz - 2])
        for c in cs:
            pl.when(jnp.logical_not(inside) if at_edge else inside)(c.start)
        fars.append((at_edge, cs))

    fars = []

    def hand_over(w_y):
        mate = z + 1 - 2 * (z % 2)
        out = []
        for d in range(1, ny):
            yy = (y + d) % ny
            k = room(1)
            out.append(remote(w_y.block(z, yy), w_y.block(z, yy), {"fs": mate * ny + y}, k, k))
            out[-1].got = remote(
                w_y.block(mate, yy), w_y.block(mate, yy), {"fs": mate * ny + y}, k, k
            )
        return out

    low_sent = []
    for turn, (h, part, yin, acc, zout, along, copies) in enumerate(units):
        if turn == 1 and nz > 3:
            forward(1, wo_z, wo_y)
        if turn == 2:
            relay(wo_z)
        for i in range(per_half):
            acc[h * per_half + i] = part[h * per_half + i, y]
        for d, c in enumerate(copies):
            with jax.named_scope("wait_y"):
                c.wait_recv()
            for i in range(per_half):
                acc[h * per_half + i] += yin[d, h * per_half + i].astype(F32)
        for i in range(per_half):
            zz = h * per_half + i
            zout[zz] = acc[zz].astype(BF16)
            c = along.to(zz)
            pl.when(zz != z)(c.start)
            low_sent.append((zz, c))

    sides = (
        (matrices[0], units[0][5], om, os_, om_new, os_new, do_all, do_z, do_y),
        (matrices[1], units[2][5], qm, qs, qm_new, qs_new, dq_all, dq_z, dq_y),
    )
    forward_far(wo_z, wo_y, False)
    for c in own[4:]:
        c.wait()
    squares = []
    for matrix, along, mean, square, mean_out, square_out, d_all, d_z, d_y in sides:
        acc, zin = matrix[7], matrix[9]
        low = acc[z]
        for zz in others:
            with jax.named_scope("wait_z"):
                along.wait(zz)
            low += zin[zz].astype(F32)
        mean_new = 0.8 * mean[...] + 0.2 * low
        square_new = 0.9 * square[...] + 0.1 * low * low
        mean_out[...] = mean_new
        square_out[...] = square_new
        direction = mean_new / jnp.sqrt(square_new)
        d_all[z, y] = direction.astype(BF16)
        for zz in others:
            launch(d_z.to(zz))
        d_y.send(z)
        squares.append(jnp.sum(direction * direction))
    lanes = lax.broadcasted_iota(jnp.int32, tile_tp.shape[1:], 1)
    tile_tp[0] = jnp.where(lanes < tile_tp.shape[2] // 2, squares[1], squares[0])

    tiles = []
    for d in range(1, nt):
        k = room(1)
        tiles.append(launch(remote(tile_tp.at[0], tile_tp.at[d], {"tp": (t + d) % nt}, k, k)))

    forward_far(wo_z, wo_y, True)

    def forward_directions(d_z, d_y):
        for zz in others:
            with jax.named_scope("wait_dz"):
                d_z.wait(zz)
            d_y.send(zz)

    forward_directions(do_z, do_y)
    late = [k for k in outward if k not in [0]]
    send_weights(wq_z, late)
    with jax.named_scope("wait_tp"):
        for c in tiles:
            c.wait_recv()
    tile_fs[0] = jnp.sum(tile_tp[...], axis=0)
    tiles = []
    for d in range(1, n):
        k = room(1)
        tiles.append(launch(remote(tile_fs.at[0], tile_fs.at[d], {"fs": (f + d) % n}, k, k)))
    forward_directions(dq_z, dq_y)
    relay(wq_z)
    handed = []
    if mated:
        for w_y in (wo_y, wq_y):
            w_y.wait(z)
            for c in hand_over(w_y):
                handed.append(launch(c))
    for k in range(2, nz - 2):
        forward(k, wo_z, wo_y)
    for k in range(1, nz - 2):
        forward(k, wq_z, wq_y)
    forward_far(wq_z, wq_y, False)
    forward_far(wq_z, wq_y, True)

    with jax.named_scope("wait_fs"):
        for c in tiles:
            c.wait_recv()
    total[...] = jnp.sum(tile_fs[...], axis=0)
    with jax.named_scope("wait_dy"):
        for zz in [z] + others:
            do_y.wait(zz)
            dq_y.wait(zz)
    with jax.named_scope("wait_wy"):
        for c in handed:
            c.got.wait_recv()
        if mated:
            wo_z.wait(others[0])
            wq_z.wait(others[0])
        for zz in others[1:] if mated else [z] + others:
            wo_y.wait(zz)
            wq_y.wait(zz)
    with jax.named_scope("wait_send"):
        for c in sent:
            c.wait_send()
    for zz, c in low_sent:
        pl.when(zz != z)(c.wait_send)
    for c in far:
        pl.when(inside)(c.wait_send)
    for here, c in ahead:
        pl.when(z == here)(c.wait_send)
    for at_edge, cs in fars:
        for c in cs:
            pl.when(jnp.logical_not(inside) if at_edge else inside)(c.wait_send)


def finish_kernel(
    nz, ny, nt,
    fq_all, fo_all, wq_all, wo_all, dq_all, do_all, total, wq, wo, qm, qs, om, os_,
    step_q_hbm, step_o_hbm, new_q_hbm, new_o_hbm, copy_q_hbm, copy_o_hbm,
    qm_hbm, qs_hbm, om_hbm, os_hbm,
    step_q, step_o, new_q, new_o, copy_q, copy_o,
    sem,
):
    f = lax.axis_index("fs")
    z, y = f // ny, f % ny
    started = []

    def put(src, dst):
        c = pltpu.make_async_copy(src, dst, sem.at[len(started)])
        c.start()
        started.append(c)

    for src, dst in ((qm, qm_hbm), (qs, qs_hbm), (om, om_hbm), (os_, os_hbm)):
        put(src, dst)
    rank = 2 * fq_all.shape[-1]
    middle = total.shape[1] // 2
    for slot, f_all, w_all, d_all, w, step, new, copy, step_hbm, new_hbm, copy_hbm in (
        (middle, fo_all, wo_all, do_all, wo, step_o, new_o, copy_o, step_o_hbm, new_o_hbm, copy_o_hbm),
        (0, fq_all, wq_all, dq_all, wq, step_q, new_q, copy_q, step_q_hbm, new_q_hbm, copy_q_hbm),
    ):
        cols = w.shape[1]
        scale = lax.rsqrt(total[...] / (rank * cols * nt) + 0.25)[:, slot:slot + 1]
        direction = d_all[...].reshape(rank, cols)
        rows = f_all.shape[3]

        def factor_rows(i, f_all=f_all):
            return jnp.concatenate([f_all[h, i].reshape(-1, rank // 2) for h in range(2)], axis=1)

        for i in range(nz):
            full = jnp.dot(
                factor_rows(i), direction, preferred_element_type=F32
            ) * scale
            at = pl.ds(i * ny * rows, ny * rows)
            old = w_all[i].reshape(ny * rows, cols).astype(F32)
            copy[at, :] = (old - 0.02 * full).astype(BF16)
            put(copy.at[at, :], copy_hbm.at[at, :])
        mine = jnp.concatenate([f_all[h, z, y] for h in range(2)], axis=1)
        own = jnp.dot(mine, direction, preferred_element_type=F32) * scale
        step[...] = own
        new[...] = w[...] - 0.02 * own
        put(step, step_hbm)
        put(new, new_hbm)
    for c in started:
        c.wait()


def on_device(
    nz, ny, nt,
    latent_in, query_cot, attn_out, mix_cot, query_weight, output_weight,
    query_factor, output_factor, query_mean, query_square, output_mean, output_square,
):
    n = nz * ny
    tokens = latent_in.shape[0]
    inv_root = 1.0 / math.sqrt(tokens * n)
    rq, cq = query_weight.shape
    ro, co = output_weight.shape
    rank = query_factor.shape[1]
    block = rank // n
    vmem = pl.BlockSpec(memory_space=pltpu.VMEM)
    hbm = pl.BlockSpec(memory_space=pltpu.HBM)
    copies = semaphores_of(nz, ny, nt)

    def exchange(*refs):
        pl.run_scoped(
            functools.partial(exchange_kernel, nz, ny, nt, inv_root, *refs),
            pltpu.SemaphoreType.DMA((CHUNKS, 4)),
            pltpu.SemaphoreType.DMA((8,)),
            pltpu.SemaphoreType.DMA((copies,)),
            pltpu.SemaphoreType.DMA((copies,)),
        )

    fq, fo, wq, wo, dq, do, total, qm, qs, om, os_ = pl.pallas_call(
        exchange,
        name="moment_exchange",
        in_specs=[hbm] * 12,
        out_specs=[vmem] * 11,
        out_shape=[
            jax.ShapeDtypeStruct((2, nz, ny, rq, rank // 2), BF16),
            jax.ShapeDtypeStruct((2, nz, ny, ro, rank // 2), BF16),
            jax.ShapeDtypeStruct((nz, ny, rq, cq), BF16),
            jax.ShapeDtypeStruct((nz, ny, ro, co), BF16),
            jax.ShapeDtypeStruct((nz, ny, block, cq), BF16),
            jax.ShapeDtypeStruct((nz, ny, block, co), BF16),
            jax.ShapeDtypeStruct((1, 128), F32),
            jax.ShapeDtypeStruct((block, cq), F32),
            jax.ShapeDtypeStruct((block, cq), F32),
            jax.ShapeDtypeStruct((block, co), F32),
            jax.ShapeDtypeStruct((block, co), F32),
        ],
        scratch_shapes=[
            pltpu.VMEM(latent_in.shape, BF16),
            pltpu.VMEM(query_cot.shape, BF16),
            pltpu.VMEM(attn_out.shape, BF16),
            pltpu.VMEM(mix_cot.shape, BF16),
            pltpu.VMEM((rq, cq), F32),
            pltpu.VMEM((ro, co), F32),
            pltpu.VMEM((block, cq), F32),
            pltpu.VMEM((block, cq), F32),
            pltpu.VMEM((block, co), F32),
            pltpu.VMEM((block, co), F32),
            pltpu.VMEM((cq, n * rq), F32),
            pltpu.VMEM((co, n * ro), F32),
            pltpu.VMEM((nz, ny, block, cq), F32),
            pltpu.VMEM((nz, ny, block, co), F32),
            pltpu.VMEM((2 * max(ny - 1, 1), nz, block, cq), BF16),
            pltpu.VMEM((2 * max(ny - 1, 1), nz, block, co), BF16),
            pltpu.VMEM((nz, block, cq), F32),
            pltpu.VMEM((nz, block, co), F32),
            pltpu.VMEM((nz, block, cq), BF16),
            pltpu.VMEM((nz, block, co), BF16),
            pltpu.VMEM((nz, block, cq), BF16),
            pltpu.VMEM((nz, block, co), BF16),
            pltpu.VMEM((nt, 1, 128), F32),
            pltpu.VMEM((n, 1, 128), F32),
            pltpu.VMEM((cq, n * rq), BF16),
            pltpu.VMEM((co, n * ro), BF16),
        ],
        compiler_params=pltpu.CompilerParams(
            collective_id=0, has_side_effects=True, vmem_limit_bytes=40 * 1024 * 1024
        ),
    )(*(pltpu.with_memory_space_constraint(a, pltpu.HBM) for a in (
        latent_in, query_cot, attn_out, mix_cot, query_weight, output_weight,
        query_factor, output_factor, query_mean, query_square, output_mean, output_square,
    )))
    shapes = (
        ((rq, cq), F32), ((ro, co), F32), ((rq, cq), F32), ((ro, co), F32),
        ((n * rq, cq), BF16), ((n * ro, co), BF16),
        ((block, cq), F32), ((block, cq), F32), ((block, co), F32), ((block, co), F32),
    )

    def finish(*refs):
        pl.run_scoped(
            functools.partial(finish_kernel, nz, ny, nt, *refs),
            pltpu.SemaphoreType.DMA((2 * nz + 8,)),
        )

    return pl.pallas_call(
        finish,
        name="finish",
        in_specs=[vmem] * 13,
        out_specs=[hbm] * 10,
        out_shape=[jax.ShapeDtypeStruct(*s) for s in shapes],
        scratch_shapes=[pltpu.VMEM(*s) for s in shapes[:6]],
        compiler_params=pltpu.CompilerParams(vmem_limit_bytes=20 * 1024 * 1024),
    )(fq, fo, wq, wo, dq, do, total, query_weight, output_weight, qm, qs, om, os_)


def solution(mesh):
    nz, ny = grid_of(mesh.shape["fs"])
    rows, both, cols = P("fs", None), P("fs", "tp"), P(None, "tp")
    return jax.shard_map(
        functools.partial(on_device, nz, ny, mesh.shape["tp"]),
        mesh=mesh,
        in_specs=(rows, both, rows, both, both, both, rows, rows, both, both, both, both),
        out_specs=(both, both, both, both, cols, cols, both, both, both, both),
        check_vma=False,
    )
```

```python
import functools
import math

import jax
import jax.numpy as jnp
from jax import lax
from jax.experimental import pallas as pl
from jax.experimental.pallas import tpu as pltpu
from jax.sharding import PartitionSpec as P

MESH = pl.DeviceIdType.MESH
BF16 = jnp.bfloat16
F32 = jnp.float32
CHUNKS = 4


def grid_of(count):
    inner = max(d for d in range(1, count + 1) if count % d == 0 and d * d <= count)
    return count // inner, inner


def semaphores_of(nz, ny, nt):
    z_kinds, y_kinds = 2 + 2 + 2 + 2, 2 + 2 + 2
    return z_kinds * nz + y_kinds * nz * (ny - 1) + 6 * (ny - 1) + 2 * ny + nt + nz * ny + 4


def over_rows(left, right):
    return lax.dot_general(left, right, (((0,), (0,)), ((), ())), preferred_element_type=F32)


def exchange_kernel(
    nz, ny, nt, inv_root,
    latent_hbm, cot_hbm, attn_hbm, mix_hbm, wq_hbm, wo_hbm, fq_hbm, fo_hbm,
    qm_hbm, qs_hbm, om_hbm, os_hbm,
    fq_all, fo_all, wq_all, wo_all, dq_all, do_all, total, qm_new, qs_new, om_new, os_new,
    latent, cot, attn, mix, wq, wo, qm, qs, om, os_, grad_q, grad_o,
    part_q, part_o, yin_q, yin_o, acc_q, acc_o, zout_q, zout_o, zin_q, zin_o,
    tile_tp, tile_fs, rounded_q, rounded_o,
    load_sem, own_sem, send_sem, recv_sem,
):
    n = nz * ny
    f = lax.axis_index("fs")
    t = lax.axis_index("tp")
    z, y = f // ny, f % ny
    half_cols = fq_all.shape[-1]
    core = t % 2
    half = pl.ds(pl.multiple_of(core * half_cols, half_cols), half_cols)
    twin = t + 1 - 2 * (t % 2)
    step = latent_hbm.shape[0] // CHUNKS

    barrier = pltpu.get_barrier_semaphore()
    for d in range(1, n):
        pl.semaphore_signal(barrier, inc=1, device_id={"fs": (f + d) % n}, device_id_type=MESH)
    for d in range(1, nt):
        pl.semaphore_signal(barrier, inc=1, device_id={"tp": (t + d) % nt}, device_id_type=MESH)

    own = [
        pltpu.make_async_copy(src, dst, own_sem.at[i])
        for i, (src, dst) in enumerate((
            (fo_hbm.at[:, half], fo_all.at[core, z, y]),
            (fq_hbm.at[:, half], fq_all.at[core, z, y]),
            (wo_hbm, wo), (wq_hbm, wq),
            (om_hbm, om), (os_hbm, os_), (qm_hbm, qm), (qs_hbm, qs),
        ))
    ]
    for c in own[:4]:
        c.start()

    def load(k, pair, sem):
        rows = pl.ds(pl.multiple_of(k * step, step), step)
        return [
            pltpu.make_async_copy(src.at[rows, :], dst.at[rows, :], load_sem.at[k, sem + i])
            for i, (src, dst) in enumerate(pair)
        ]

    pair_o = ((attn_hbm, attn), (mix_hbm, mix))
    pair_q = ((latent_hbm, latent), (cot_hbm, cot))
    with jax.named_scope("own"):
        for c in own[:4]:
            c.wait()
    for k in range(CHUNKS):
        for c in load(k, pair_q, 2):
            c.start()
    for k in range(CHUNKS):
        for c in load(k, pair_o, 0):
            c.start()
    for c in own[4:]:
        c.start()
    wo_all[z, y] = wo[...].astype(BF16)
    wq_all[z, y] = wq[...].astype(BF16)
    with jax.named_scope("barrier"):
        pl.semaphore_wait(barrier, n - 1 + nt - 1)

    used = [0]
    sent = []

    def room(count):
        at = used[0]
        used[0] = at + count
        return at

    def remote(src, dst, device, at, to):
        return pltpu.make_async_remote_copy(
            src_ref=src, dst_ref=dst, send_sem=send_sem.at[at], recv_sem=recv_sem.at[to],
            device_id=device, device_id_type=MESH,
        )

    def launch(c):
        c.start()
        sent.append(c)
        return c

    lower, upper = z, nz - 1 - z
    both = jnp.minimum(lower, upper)

    def near(k):
        paired = k < 2 * both
        away = jnp.where(paired, k // 2 + 1, k - both + 1)
        down = jnp.where(paired, (k + z) % 2 == 1, lower > upper)
        return jnp.where(down, z - away, z + away)

    others = [near(k) for k in range(nz - 1)]

    class Along:
        def __init__(self, block, landing=None):
            self.block, self.landing, self.at = block, landing or block, room(nz)

        def to(self, zz):
            return remote(
                self.block(z) if self.landing is self.block else self.block(zz), self.landing(z),
                {"fs": zz * ny + y}, self.at + zz, self.at + z,
            )

        def wait(self, zz):
            remote(
                self.landing(zz), self.landing(zz), {"fs": zz * ny + y}, self.at + zz, self.at + zz
            ).wait_recv()

    class Across:
        def __init__(self, block):
            self.block, self.at = block, room(nz * (ny - 1))

        def copies(self, zz):
            ks = [self.at + (d - 1) * nz + zz for d in range(1, ny)]
            return [
                remote(self.block(zz, y), self.block(zz, y), {"fs": z * ny + (y + d) % ny}, k, k)
                for d, k in zip(range(1, ny), ks)
            ]

        def send(self, zz):
            for c in self.copies(zz):
                launch(c)

        def wait(self, zz):
            for d in range(1, ny):
                k = self.at + (d - 1) * nz + zz
                block = self.block(zz, (y + ny - d) % ny)
                remote(block, block, {"fs": z * ny + (y + d) % ny}, k, k).wait_recv()

    fo_z = Along(lambda zz: fo_all.at[core, zz, y])
    fq_z = Along(lambda zz: fq_all.at[core, zz, y])
    fo_y = Across(lambda zz, yy: fo_all.at[core, zz, yy])
    fq_y = Across(lambda zz, yy: fq_all.at[core, zz, yy])
    wo_z = Along(lambda zz: wo_all.at[zz, y])
    wq_z = Along(lambda zz: wq_all.at[zz, y])
    wo_y = Across(lambda zz, yy: wo_all.at[zz, yy])
    wq_y = Across(lambda zz, yy: wq_all.at[zz, yy])
    do_z = Along(lambda zz: do_all.at[zz, y])
    dq_z = Along(lambda zz: dq_all.at[zz, y])
    do_y = Across(lambda zz, yy: do_all.at[zz, yy])
    dq_y = Across(lambda zz, yy: dq_all.at[zz, yy])

    for fac_z, fac_y in ((fq_z, fq_y), (fo_z, fo_y)):
        for zz in others:
            launch(fac_z.to(zz))
        fac_y.send(z)
    wo_y.send(z)

    through = nz >= 3
    mated = nz % 2 == 0
    inside = jnp.logical_and(z > 0, z < nz - 1)
    far = []

    def send_weights(w_z, ks, relayed=False):
        for k in ks:
            c = w_z.to(others[k])
            if relayed and through and k == nz - 2:
                far.append(c)
                pl.when(inside)(c.start)
            else:
                launch(c)

    outward = list(reversed(range(nz - 1)))

    def product(k, pair, sem, out):
        for c in load(k, pair, sem):
            c.wait()
        rows = pl.ds(pl.multiple_of(k * step, step), step)
        new = over_rows(pair[1][1][rows, :], pair[0][1][rows, :])
        out[...] += new

    def products(lo, hi, pair, sem, out):
        @pl.loop(lo, hi)
        def _(k):
            product(k, pair, sem, out)

    grad_o[...] = jnp.zeros_like(grad_o)
    grad_q[...] = jnp.zeros_like(grad_q)
    swaps = {}

    def swap(all_, yy):
        block = all_.at[core, :, yy]
        k = room(1)
        return launch(remote(block, block, {"tp": twin}, k, k))

    done = 0

    def more_o(upto):
        nonlocal done
        if done < upto:
            with jax.named_scope("prod_o"):
                products(done, upto, pair_o, 0, grad_o)
            done = upto

    with jax.named_scope("prod_q"):
        products(0, CHUNKS, pair_q, 2, grad_q)
    more_o(1)
    for zz in others:
        with jax.named_scope("wait_fqz"):
            fq_z.wait(zz)
        fq_y.send(zz)
    swaps["q"] = [swap(fq_all, y)]
    send_weights(wo_z, outward, True)
    for k, zz in enumerate(others):
        if k == 0:
            more_o(2)
        with jax.named_scope("wait_foz"):
            fo_z.wait(zz)
        fo_y.send(zz)
    swaps["o"] = [swap(fo_all, y)]
    more_o(CHUNKS - 1)

    rank = 2 * half_cols
    block = rank // n
    per_half = nz // 2

    def project(h, factor_all, grad, part):
        factor = factor_all[h].reshape(-1, half_cols)
        low = lax.dot_general(
            factor, grad[...], (((0,), (1,)), ((), ())), preferred_element_type=F32
        ) * inv_root
        for i in range(per_half):
            for j in range(ny):
                at = (i * ny + j) * block
                part[h * per_half + i, j] = low[at:at + block, :]

    matrices = (
        ("q", fq_all, fq_y, grad_q, rounded_q, part_q, yin_q, acc_q, zout_q, zin_q),
        ("o", fo_all, fo_y, grad_o, rounded_o, part_o, yin_o, acc_o, zout_o, zin_o),
    )
    units = []
    for name, all_, fac_y, grad, rounded, part, yin, acc, zout, zin in matrices:
        if name == "o":
            wq_y.send(z)
            more_o(CHUNKS)
        rounded[...] = grad[...].astype(BF16)
        along = Along(lambda zz, zout=zout: zout.at[zz], lambda zz, zin=zin: zin.at[zz])
        with jax.named_scope("wait_fy"):
            for zz in [z] + others:
                fac_y.wait(zz)
        for d in range(1, ny):
            swaps[name].append(swap(all_, (y + ny - d) % ny))
        for turn, h in enumerate((core, 1 - core)):
            if turn:
                with jax.named_scope("wait_swap"):
                    for c in swaps[name]:
                        c.wait_recv()
            with jax.named_scope("project"):
                project(h, all_, rounded, part)
            rows = pl.ds(h * per_half, per_half)
            copies = []
            for d in range(1, ny):
                yy = (y + d) % ny
                for i in range(per_half):
                    yin[ny - 1 + d - 1, h * per_half + i] = part[h * per_half + i, yy].astype(BF16)
                k = room(1)
                copies.append(launch(remote(
                    yin.at[ny - 1 + d - 1, rows], yin.at[d - 1, rows], {"fs": z * ny + yy}, k, k
                )))
            units.append((h, part, yin, acc, zout, along, copies))

    def forward(k, w_z, w_y):
        with jax.named_scope("wait_wz"):
            w_z.wait(others[k])
        w_y.send(others[k])

    if nz > 1 and not mated:
        forward(0, wo_z, wo_y)
        forward(0, wq_z, wq_y)

    ahead = []

    def relay(w_z):
        if not through:
            return
        mine = []
        for edge, here in ((0, nz - 2), (nz - 1, 1)):
            k = room(1)
            mine.append((here, remote(
                w_z.block(edge), w_z.block(edge), {"fs": (nz - 1 - edge) * ny + y},
                k, w_z.at + edge,
            )))

        @pl.when(inside)
        def _():
            with jax.named_scope("wait_far"):
                w_z.wait(others[nz - 2])
        for here, c in mine:
            pl.when(z == here)(c.start)
        ahead.extend(mine)

    def forward_far(w_z, w_y, at_edge):
        if not through:
            return
        if at_edge:
            @pl.when(jnp.logical_not(inside))
            def _():
                with jax.named_scope("wait_wz_last"):
                    w_z.wait(others[nz - 2])
        cs = w_y.copies(others[nz - 2])
        for c in cs:
            pl.when(jnp.logical_not(inside) if at_edge else inside)(c.start)
        fars.append((at_edge, cs))

    fars = []

    def hand_over(w_y):
        mate = z + 1 - 2 * (z % 2)
        out = []
        for d in range(1, ny):
            yy = (y + d) % ny
            k = room(1)
            out.append(remote(w_y.block(z, yy), w_y.block(z, yy), {"fs": mate * ny + y}, k, k))
            out[-1].got = remote(
                w_y.block(mate, yy), w_y.block(mate, yy), {"fs": mate * ny + y}, k, k
            )
        return out

    low_sent = []
    for turn, (h, part, yin, acc, zout, along, copies) in enumerate(units):
        if turn == 2:
            relay(wo_z)
        if turn == 3 and nz > 3:
            forward(1, wo_z, wo_y)
        for i in range(per_half):
            acc[h * per_half + i] = part[h * per_half + i, y]
        for d, c in enumerate(copies):
            with jax.named_scope("wait_y"):
                c.wait_recv()
            for i in range(per_half):
                acc[h * per_half + i] += yin[d, h * per_half + i].astype(F32)
        for i in range(per_half):
            zz = h * per_half + i
            zout[zz] = acc[zz].astype(BF16)
            c = along.to(zz)
            pl.when(zz != z)(c.start)
            low_sent.append((zz, c))

    sides = (
        (matrices[0], units[0][5], qm, qs, qm_new, qs_new, dq_all, dq_z, dq_y),
        (matrices[1], units[2][5], om, os_, om_new, os_new, do_all, do_z, do_y),
    )
    forward_far(wo_z, wo_y, False)
    for c in own[4:]:
        c.wait()
    squares = []
    for matrix, along, mean, square, mean_out, square_out, d_all, d_z, d_y in sides:
        acc, zin = matrix[7], matrix[9]
        low = acc[z]
        for zz in others:
            with jax.named_scope("wait_z"):
                along.wait(zz)
            low += zin[zz].astype(F32)
        mean_new = 0.8 * mean[...] + 0.2 * low
        square_new = 0.9 * square[...] + 0.1 * low * low
        mean_out[...] = mean_new
        square_out[...] = square_new
        direction = mean_new / jnp.sqrt(square_new)
        d_all[z, y] = direction.astype(BF16)
        for zz in others:
            launch(d_z.to(zz))
        d_y.send(z)
        squares.append(jnp.sum(direction * direction))
        if len(squares) == 1:
            forward_far(wo_z, wo_y, True)
    lanes = lax.broadcasted_iota(jnp.int32, tile_tp.shape[1:], 1)
    tile_tp[0] = jnp.where(lanes < tile_tp.shape[2] // 2, squares[0], squares[1])

    tiles = []
    for d in range(1, nt):
        k = room(1)
        tiles.append(launch(remote(tile_tp.at[0], tile_tp.at[d], {"tp": (t + d) % nt}, k, k)))
    send_weights(wq_z, outward)

    def forward_directions(d_z, d_y):
        for zz in others:
            with jax.named_scope("wait_dz"):
                d_z.wait(zz)
            d_y.send(zz)

    handed = []

    def hand(w_y):
        if mated:
            w_y.wait(z)
            for c in hand_over(w_y):
                handed.append(launch(c))

    hand(wo_y)
    forward_directions(dq_z, dq_y)
    with jax.named_scope("wait_tp"):
        for c in tiles:
            c.wait_recv()
    tile_fs[0] = jnp.sum(tile_tp[...], axis=0)
    tiles = []
    for d in range(1, n):
        k = room(1)
        tiles.append(launch(remote(tile_fs.at[0], tile_fs.at[d], {"fs": (f + d) % n}, k, k)))
    forward_directions(do_z, do_y)
    hand(wq_y)
    for k in range(2, nz - 2):
        forward(k, wo_z, wo_y)
    for k in range(1, nz - 1):
        forward(k, wq_z, wq_y)
    with jax.named_scope("wait_fs"):
        for c in tiles:
            c.wait_recv()
    total[...] = jnp.sum(tile_fs[...], axis=0)
    with jax.named_scope("wait_dy"):
        for zz in [z] + others:
            do_y.wait(zz)
            dq_y.wait(zz)
    with jax.named_scope("wait_wy"):
        for c in handed:
            c.got.wait_recv()
        if mated:
            wo_z.wait(others[0])
            wq_z.wait(others[0])
        for zz in others[1:] if mated else [z] + others:
            wo_y.wait(zz)
            wq_y.wait(zz)
    with jax.named_scope("wait_send"):
        for c in sent:
            c.wait_send()
    for zz, c in low_sent:
        pl.when(zz != z)(c.wait_send)
    for c in far:
        pl.when(inside)(c.wait_send)
    for here, c in ahead:
        pl.when(z == here)(c.wait_send)
    for at_edge, cs in fars:
        for c in cs:
            pl.when(jnp.logical_not(inside) if at_edge else inside)(c.wait_send)


def finish_kernel(
    nz, ny, nt,
    fq_all, fo_all, wq_all, wo_all, dq_all, do_all, total, wq, wo, qm, qs, om, os_,
    step_q_hbm, step_o_hbm, new_q_hbm, new_o_hbm, copy_q_hbm, copy_o_hbm,
    qm_hbm, qs_hbm, om_hbm, os_hbm,
    step_q, step_o, new_q, new_o, copy_q, copy_o,
    sem,
):
    f = lax.axis_index("fs")
    z, y = f // ny, f % ny
    started = []

    def put(src, dst):
        c = pltpu.make_async_copy(src, dst, sem.at[len(started)])
        c.start()
        started.append(c)

    for src, dst in ((qm, qm_hbm), (qs, qs_hbm), (om, om_hbm), (os_, os_hbm)):
        put(src, dst)
    rank = 2 * fq_all.shape[-1]
    middle = total.shape[1] // 2
    for slot, f_all, w_all, d_all, w, step, new, copy, step_hbm, new_hbm, copy_hbm in (
        (middle, fo_all, wo_all, do_all, wo, step_o, new_o, copy_o, step_o_hbm, new_o_hbm, copy_o_hbm),
        (0, fq_all, wq_all, dq_all, wq, step_q, new_q, copy_q, step_q_hbm, new_q_hbm, copy_q_hbm),
    ):
        cols = w.shape[1]
        scale = lax.rsqrt(total[...] / (rank * cols * nt) + 0.25)[:, slot:slot + 1]
        direction = d_all[...].reshape(rank, cols)
        rows = f_all.shape[3]

        def factor_rows(i, f_all=f_all):
            return jnp.concatenate([f_all[h, i].reshape(-1, rank // 2) for h in range(2)], axis=1)

        for i in range(nz):
            full = jnp.dot(
                factor_rows(i), direction, preferred_element_type=F32
            ) * scale
            at = pl.ds(i * ny * rows, ny * rows)
            old = w_all[i].reshape(ny * rows, cols).astype(F32)
            copy[at, :] = (old - 0.02 * full).astype(BF16)
            put(copy.at[at, :], copy_hbm.at[at, :])
        mine = jnp.concatenate([f_all[h, z, y] for h in range(2)], axis=1)
        own = jnp.dot(mine, direction, preferred_element_type=F32) * scale
        step[...] = own
        new[...] = w[...] - 0.02 * own
        put(step, step_hbm)
        put(new, new_hbm)
    for c in started:
        c.wait()


def on_device(
    nz, ny, nt,
    latent_in, query_cot, attn_out, mix_cot, query_weight, output_weight,
    query_factor, output_factor, query_mean, query_square, output_mean, output_square,
):
    n = nz * ny
    tokens = latent_in.shape[0]
    inv_root = 1.0 / math.sqrt(tokens * n)
    rq, cq = query_weight.shape
    ro, co = output_weight.shape
    rank = query_factor.shape[1]
    block = rank // n
    vmem = pl.BlockSpec(memory_space=pltpu.VMEM)
    hbm = pl.BlockSpec(memory_space=pltpu.HBM)
    copies = semaphores_of(nz, ny, nt)

    def exchange(*refs):
        pl.run_scoped(
            functools.partial(exchange_kernel, nz, ny, nt, inv_root, *refs),
            pltpu.SemaphoreType.DMA((CHUNKS, 4)),
            pltpu.SemaphoreType.DMA((8,)),
            pltpu.SemaphoreType.DMA((copies,)),
            pltpu.SemaphoreType.DMA((copies,)),
        )

    fq, fo, wq, wo, dq, do, total, qm, qs, om, os_ = pl.pallas_call(
        exchange,
        name="moment_exchange",
        in_specs=[hbm] * 12,
        out_specs=[vmem] * 11,
        out_shape=[
            jax.ShapeDtypeStruct((2, nz, ny, rq, rank // 2), BF16),
            jax.ShapeDtypeStruct((2, nz, ny, ro, rank // 2), BF16),
            jax.ShapeDtypeStruct((nz, ny, rq, cq), BF16),
            jax.ShapeDtypeStruct((nz, ny, ro, co), BF16),
            jax.ShapeDtypeStruct((nz, ny, block, cq), BF16),
            jax.ShapeDtypeStruct((nz, ny, block, co), BF16),
            jax.ShapeDtypeStruct((1, 128), F32),
            jax.ShapeDtypeStruct((block, cq), F32),
            jax.ShapeDtypeStruct((block, cq), F32),
            jax.ShapeDtypeStruct((block, co), F32),
            jax.ShapeDtypeStruct((block, co), F32),
        ],
        scratch_shapes=[
            pltpu.VMEM(latent_in.shape, BF16),
            pltpu.VMEM(query_cot.shape, BF16),
            pltpu.VMEM(attn_out.shape, BF16),
            pltpu.VMEM(mix_cot.shape, BF16),
            pltpu.VMEM((rq, cq), F32),
            pltpu.VMEM((ro, co), F32),
            pltpu.VMEM((block, cq), F32),
            pltpu.VMEM((block, cq), F32),
            pltpu.VMEM((block, co), F32),
            pltpu.VMEM((block, co), F32),
            pltpu.VMEM((cq, n * rq), F32),
            pltpu.VMEM((co, n * ro), F32),
            pltpu.VMEM((nz, ny, block, cq), F32),
            pltpu.VMEM((nz, ny, block, co), F32),
            pltpu.VMEM((2 * max(ny - 1, 1), nz, block, cq), BF16),
            pltpu.VMEM((2 * max(ny - 1, 1), nz, block, co), BF16),
            pltpu.VMEM((nz, block, cq), F32),
            pltpu.VMEM((nz, block, co), F32),
            pltpu.VMEM((nz, block, cq), BF16),
            pltpu.VMEM((nz, block, co), BF16),
            pltpu.VMEM((nz, block, cq), BF16),
            pltpu.VMEM((nz, block, co), BF16),
            pltpu.VMEM((nt, 1, 128), F32),
            pltpu.VMEM((n, 1, 128), F32),
            pltpu.VMEM((cq, n * rq), BF16),
            pltpu.VMEM((co, n * ro), BF16),
        ],
        compiler_params=pltpu.CompilerParams(
            collective_id=0, has_side_effects=True, vmem_limit_bytes=40 * 1024 * 1024
        ),
    )(*(pltpu.with_memory_space_constraint(a, pltpu.HBM) for a in (
        latent_in, query_cot, attn_out, mix_cot, query_weight, output_weight,
        query_factor, output_factor, query_mean, query_square, output_mean, output_square,
    )))
    shapes = (
        ((rq, cq), F32), ((ro, co), F32), ((rq, cq), F32), ((ro, co), F32),
        ((n * rq, cq), BF16), ((n * ro, co), BF16),
        ((block, cq), F32), ((block, cq), F32), ((block, co), F32), ((block, co), F32),
    )

    def finish(*refs):
        pl.run_scoped(
            functools.partial(finish_kernel, nz, ny, nt, *refs),
            pltpu.SemaphoreType.DMA((2 * nz + 8,)),
        )

    return pl.pallas_call(
        finish,
        name="finish",
        in_specs=[vmem] * 13,
        out_specs=[hbm] * 10,
        out_shape=[jax.ShapeDtypeStruct(*s) for s in shapes],
        scratch_shapes=[pltpu.VMEM(*s) for s in shapes[:6]],
        compiler_params=pltpu.CompilerParams(vmem_limit_bytes=20 * 1024 * 1024),
    )(fq, fo, wq, wo, dq, do, total, query_weight, output_weight, qm, qs, om, os_)


def solution(mesh):
    nz, ny = grid_of(mesh.shape["fs"])
    rows, both, cols = P("fs", None), P("fs", "tp"), P(None, "tp")
    return jax.shard_map(
        functools.partial(on_device, nz, ny, mesh.shape["tp"]),
        mesh=mesh,
        in_specs=(rows, both, rows, both, both, both, rows, rows, both, both, both, both),
        out_specs=(both, both, both, both, cols, cols, both, both, both, both),
        check_vma=False,
    )
```

```python
import functools
import math

import jax
import jax.numpy as jnp
from jax import lax
from jax.experimental import pallas as pl
from jax.experimental.pallas import tpu as pltpu
from jax.sharding import PartitionSpec as P

MESH = pl.DeviceIdType.MESH
BF16 = jnp.bfloat16
F32 = jnp.float32
CHUNKS = 4


def grid_of(count):
    inner = max(d for d in range(1, count + 1) if count % d == 0 and d * d <= count)
    return count // inner, inner


def semaphores_of(nz, ny, nt):
    z_kinds, y_kinds = 2 + 2 + 2 + 2, 2 + 2 + 2
    return z_kinds * nz + y_kinds * nz * (ny - 1) + 6 * (ny - 1) + 2 * ny + nt + nz * ny + 4 + ny * nt


def over_rows(left, right):
    return lax.dot_general(left, right, (((0,), (0,)), ((), ())), preferred_element_type=F32)


def exchange_kernel(
    nz, ny, nt, inv_root,
    latent_hbm, cot_hbm, attn_hbm, mix_hbm, wq_hbm, wo_hbm, fq_hbm, fo_hbm,
    qm_hbm, qs_hbm, om_hbm, os_hbm,
    fq_all, fo_all, wq_all, wo_all, dq_all, do_all, total, qm_new, qs_new, om_new, os_new,
    latent, cot, attn, mix, wq, wo, qm, qs, om, os_, grad_q, grad_o,
    part_q, part_o, yin_q, yin_o, acc_q, acc_o, zout_q, zout_o, zin_q, zin_o,
    tile_tp, tile_fs, rounded_q, rounded_o,
    load_sem, own_sem, send_sem, recv_sem,
):
    n = nz * ny
    f = lax.axis_index("fs")
    t = lax.axis_index("tp")
    z, y = f // ny, f % ny
    half_cols = fq_all.shape[-1]
    core = t % 2
    half = pl.ds(pl.multiple_of(core * half_cols, half_cols), half_cols)
    twin = t + 1 - 2 * (t % 2)
    step = latent_hbm.shape[0] // CHUNKS
    shares = nt // 2 if fo_hbm.shape[0] % (16 * (nt // 2)) == 0 else 1
    share_rows = fo_hbm.shape[0] // shares
    share = pl.ds(pl.multiple_of((t // 2) % shares * share_rows, share_rows), share_rows)

    barrier = pltpu.get_barrier_semaphore()
    for d in range(1, n):
        pl.semaphore_signal(barrier, inc=1, device_id={"fs": (f + d) % n}, device_id_type=MESH)
    for d in range(1, nt):
        pl.semaphore_signal(barrier, inc=1, device_id={"tp": (t + d) % nt}, device_id_type=MESH)

    own = [
        pltpu.make_async_copy(src, dst, own_sem.at[i])
        for i, (src, dst) in enumerate((
            (fo_hbm.at[share, half], fo_all.at[core, z, y, share]),
            (fq_hbm.at[:, half], fq_all.at[core, z, y]),
            (wo_hbm, wo), (wq_hbm, wq),
            (om_hbm, om), (os_hbm, os_), (qm_hbm, qm), (qs_hbm, qs),
        ))
    ]
    for c in own[:4]:
        c.start()

    def load(k, pair, sem):
        rows = pl.ds(pl.multiple_of(k * step, step), step)
        return [
            pltpu.make_async_copy(src.at[rows, :], dst.at[rows, :], load_sem.at[k, sem + i])
            for i, (src, dst) in enumerate(pair)
        ]

    pair_o = ((attn_hbm, attn), (mix_hbm, mix))
    pair_q = ((latent_hbm, latent), (cot_hbm, cot))
    with jax.named_scope("own"):
        for c in own[:4]:
            c.wait()
    for k in range(CHUNKS):
        for c in load(k, pair_q, 2):
            c.start()
    for k in range(CHUNKS):
        for c in load(k, pair_o, 0):
            c.start()
    for c in own[4:]:
        c.start()
    wo_all[z, y] = wo[...].astype(BF16)
    wq_all[z, y] = wq[...].astype(BF16)
    with jax.named_scope("barrier"):
        pl.semaphore_wait(barrier, n - 1 + nt - 1)

    used = [0]
    sent = []

    def room(count):
        at = used[0]
        used[0] = at + count
        return at

    def remote(src, dst, device, at, to):
        return pltpu.make_async_remote_copy(
            src_ref=src, dst_ref=dst, send_sem=send_sem.at[at], recv_sem=recv_sem.at[to],
            device_id=device, device_id_type=MESH,
        )

    def launch(c):
        c.start()
        sent.append(c)
        return c

    lower, upper = z, nz - 1 - z
    both = jnp.minimum(lower, upper)

    def near(k):
        paired = k < 2 * both
        away = jnp.where(paired, k // 2 + 1, k - both + 1)
        down = jnp.where(paired, (k + z) % 2 == 1, lower > upper)
        return jnp.where(down, z - away, z + away)

    others = [near(k) for k in range(nz - 1)]

    class Along:
        def __init__(self, block, landing=None):
            self.block, self.landing, self.at = block, landing or block, room(nz)

        def to(self, zz):
            return remote(
                self.block(z) if self.landing is self.block else self.block(zz), self.landing(z),
                {"fs": zz * ny + y}, self.at + zz, self.at + z,
            )

        def wait(self, zz):
            remote(
                self.landing(zz), self.landing(zz), {"fs": zz * ny + y}, self.at + zz, self.at + zz
            ).wait_recv()

    class Across:
        def __init__(self, block):
            self.block, self.at = block, room(nz * (ny - 1))

        def copies(self, zz):
            ks = [self.at + (d - 1) * nz + zz for d in range(1, ny)]
            return [
                remote(self.block(zz, y), self.block(zz, y), {"fs": z * ny + (y + d) % ny}, k, k)
                for d, k in zip(range(1, ny), ks)
            ]

        def send(self, zz):
            for c in self.copies(zz):
                launch(c)

        def wait(self, zz):
            for d in range(1, ny):
                k = self.at + (d - 1) * nz + zz
                block = self.block(zz, (y + ny - d) % ny)
                remote(block, block, {"fs": z * ny + (y + d) % ny}, k, k).wait_recv()

    fo_z = Along(lambda zz: fo_all.at[core, zz, y, share])
    fq_z = Along(lambda zz: fq_all.at[core, zz, y])
    fo_y = Across(lambda zz, yy: fo_all.at[core, zz, yy, share])
    fq_y = Across(lambda zz, yy: fq_all.at[core, zz, yy])
    wo_z = Along(lambda zz: wo_all.at[zz, y])
    wq_z = Along(lambda zz: wq_all.at[zz, y])
    wo_y = Across(lambda zz, yy: wo_all.at[zz, yy])
    wq_y = Across(lambda zz, yy: wq_all.at[zz, yy])
    do_z = Along(lambda zz: do_all.at[zz, y])
    dq_z = Along(lambda zz: dq_all.at[zz, y])
    do_y = Across(lambda zz, yy: do_all.at[zz, yy])
    dq_y = Across(lambda zz, yy: dq_all.at[zz, yy])

    for fac_z, fac_y in ((fq_z, fq_y), (fo_z, fo_y)):
        for zz in others:
            launch(fac_z.to(zz))
        fac_y.send(z)
    wo_y.send(z)

    through = nz >= 3
    mated = nz % 2 == 0
    inside = jnp.logical_and(z > 0, z < nz - 1)
    far = []

    def send_weights(w_z):
        for k, zz in enumerate(others):
            c = w_z.to(zz)
            if through and k > 0:
                free = jnp.logical_or(
                    jnp.logical_and(zz > 0, zz < nz - 1), jnp.logical_or(zz == z + 1, zz == z - 1)
                )
                far.append((free, c))
                pl.when(free)(c.start)
            else:
                launch(c)

    def product(k, pair, sem, out):
        for c in load(k, pair, sem):
            c.wait()
        rows = pl.ds(pl.multiple_of(k * step, step), step)
        new = over_rows(pair[1][1][rows, :], pair[0][1][rows, :])
        out[...] += new

    def products(lo, hi, pair, sem, out):
        @pl.loop(lo, hi)
        def _(k):
            product(k, pair, sem, out)

    grad_o[...] = jnp.zeros_like(grad_o)
    grad_q[...] = jnp.zeros_like(grad_q)
    swaps = {}

    def swap(all_, yy):
        block = all_.at[core, :, yy]
        k = room(1)
        return launch(remote(block, block, {"tp": twin}, k, k))

    def to_chips(yy):
        out = []
        for d in range(1, shares):
            block = fo_all.at[core, :, yy, share]
            k = room(1)
            out.append(launch(remote(block, block, {"tp": (t + 2 * d) % nt}, k, k)))
        return out

    def arrived(copies):
        with jax.named_scope("wait_x"):
            for c in copies:
                c.wait_recv()

    done = 0

    def more_o(upto):
        nonlocal done
        if done < upto:
            with jax.named_scope("prod_o"):
                products(done, upto, pair_o, 0, grad_o)
            done = upto

    with jax.named_scope("prod_q"):
        products(0, CHUNKS, pair_q, 2, grad_q)
    more_o(1)
    for zz in others:
        with jax.named_scope("wait_fqz"):
            fq_z.wait(zz)
        fq_y.send(zz)
    swaps["q"] = [swap(fq_all, y)]
    send_weights(wo_z)
    send_weights(wq_z)
    for k, zz in enumerate(others):
        with jax.named_scope("wait_foz"):
            fo_z.wait(zz)
        fo_y.send(zz)
    near_o = to_chips(y)
    more_o(CHUNKS - 1)
    across_o = []

    rank = 2 * half_cols
    block = rank // n
    per_half = nz // 2

    def project(h, factor_all, grad, part):
        factor = factor_all[h].reshape(-1, half_cols)
        low = lax.dot_general(
            factor, grad[...], (((0,), (1,)), ((), ())), preferred_element_type=F32
        ) * inv_root
        for i in range(per_half):
            for j in range(ny):
                at = (i * ny + j) * block
                part[h * per_half + i, j] = low[at:at + block, :]

    matrices = (
        ("q", fq_all, fq_y, grad_q, rounded_q, part_q, yin_q, acc_q, zout_q, zin_q),
        ("o", fo_all, fo_y, grad_o, rounded_o, part_o, yin_o, acc_o, zout_o, zin_o),
    )
    ahead = []

    def relay(w_z, ks):
        for k in ks if through else ():
            mine = []
            for edge, here in ((0, 1), (nz - 1, nz - 2)):
                at = room(1)
                mine.append((here, remote(
                    w_z.block(others[k]), w_z.block(others[k]), {"fs": edge * ny + y},
                    at, w_z.at + others[k],
                )))
            with jax.named_scope("wait_far"):
                pl.when(inside)(lambda: w_z.wait(others[k]))
            for here, c in mine:
                pl.when(z == here)(c.start)
            ahead.extend(mine)

    def pass_on(w_z, w_y, k):
        with jax.named_scope("wait_edge"):
            if through:
                pl.when(jnp.logical_not(inside))(lambda: w_z.wait(others[k]))
            else:
                w_z.wait(others[k])
        w_y.send(others[k])

    units = []
    for name, all_, fac_y, grad, rounded, part, yin, acc, zout, zin in matrices:
        if name == "o":
            wq_y.send(z)
            more_o(CHUNKS)
            arrived(across_o)
        rounded[...] = grad[...].astype(BF16)
        along = Along(lambda zz, zout=zout: zout.at[zz], lambda zz, zin=zin: zin.at[zz])
        if name == "q":
            with jax.named_scope("wait_fy"):
                for zz in [z] + others:
                    fac_y.wait(zz)
        for d in range(1, ny):
            swaps[name].append(swap(all_, (y + ny - d) % ny))
        for turn, h in enumerate((core, 1 - core)):
            if turn and name == "q":
                with jax.named_scope("wait_foy"):
                    for zz in [z] + others:
                        fo_y.wait(zz)
                for d in range(1, ny):
                    across_o += to_chips((y + ny - d) % ny)
                arrived(near_o)
                swaps["o"] = [swap(fo_all, y)]
            if turn:
                with jax.named_scope("wait_swap"):
                    for c in swaps[name]:
                        c.wait_recv()
            with jax.named_scope("project"):
                project(h, all_, rounded, part)
            rows = pl.ds(h * per_half, per_half)
            copies = []
            for d in range(1, ny):
                yy = (y + d) % ny
                for i in range(per_half):
                    yin[ny - 1 + d - 1, h * per_half + i] = part[h * per_half + i, yy].astype(BF16)
                k = room(1)
                copies.append(launch(remote(
                    yin.at[ny - 1 + d - 1, rows], yin.at[d - 1, rows], {"fs": z * ny + yy}, k, k
                )))
            if name == "q" and turn == 1:
                relay(wo_z, range(1, min(2, nz - 1)))
            if name == "o" and turn == 0:
                relay(wo_z, range(2, nz - 1))
            units.append((h, part, yin, acc, zout, along, copies))

    def forward(k, w_z, w_y):
        with jax.named_scope("wait_wz"):
            w_z.wait(others[k])
        w_y.send(others[k])

    if nz > 1 and not mated:
        forward(0, wo_z, wo_y)
        forward(0, wq_z, wq_y)

    def hand_over(w_y):
        mate = z + 1 - 2 * (z % 2)
        out = []
        for d in range(1, ny):
            yy = (y + d) % ny
            k = room(1)
            out.append(remote(w_y.block(z, yy), w_y.block(z, yy), {"fs": mate * ny + y}, k, k))
            out[-1].got = remote(
                w_y.block(mate, yy), w_y.block(mate, yy), {"fs": mate * ny + y}, k, k
            )
        return out

    low_sent = []
    for turn, (h, part, yin, acc, zout, along, copies) in enumerate(units):
        if turn == 3:
            relay(wq_z, range(1, nz - 1))
        if turn == 3 and nz > 2:
            pass_on(wo_z, wo_y, 1)
        for i in range(per_half):
            acc[h * per_half + i] = part[h * per_half + i, y]
        for d, c in enumerate(copies):
            with jax.named_scope("wait_y"):
                c.wait_recv()
            for i in range(per_half):
                acc[h * per_half + i] += yin[d, h * per_half + i].astype(F32)
        for i in range(per_half):
            zz = h * per_half + i
            zout[zz] = acc[zz].astype(BF16)
            c = along.to(zz)
            pl.when(zz != z)(c.start)
            low_sent.append((zz, c))

    sides = (
        (matrices[0], units[0][5], qm, qs, qm_new, qs_new, dq_all, dq_z, dq_y),
        (matrices[1], units[2][5], om, os_, om_new, os_new, do_all, do_z, do_y),
    )
    for k in range(2, nz - 1):
        pass_on(wo_z, wo_y, k)
    for c in own[4:]:
        c.wait()
    squares = []
    for matrix, along, mean, square, mean_out, square_out, d_all, d_z, d_y in sides:
        acc, zin = matrix[7], matrix[9]
        low = acc[z]
        for zz in others:
            with jax.named_scope("wait_z"):
                along.wait(zz)
            low += zin[zz].astype(F32)
        mean_new = 0.8 * mean[...] + 0.2 * low
        square_new = 0.9 * square[...] + 0.1 * low * low
        mean_out[...] = mean_new
        square_out[...] = square_new
        direction = mean_new / jnp.sqrt(square_new)
        d_all[z, y] = direction.astype(BF16)
        for zz in others:
            launch(d_z.to(zz))
        d_y.send(z)
        squares.append(jnp.sum(direction * direction))
        if len(squares) == 1:
            pass
    lanes = lax.broadcasted_iota(jnp.int32, tile_tp.shape[1:], 1)
    tile_tp[0] = jnp.where(lanes < tile_tp.shape[2] // 2, squares[0], squares[1])

    tiles = []
    for d in range(1, nt):
        k = room(1)
        tiles.append(launch(remote(tile_tp.at[0], tile_tp.at[d], {"tp": (t + d) % nt}, k, k)))

    def forward_directions(d_z, d_y):
        for zz in others:
            with jax.named_scope("wait_dz"):
                d_z.wait(zz)
            d_y.send(zz)

    handed = []

    def hand(w_y):
        if mated:
            w_y.wait(z)
            for c in hand_over(w_y):
                handed.append(launch(c))

    forward_directions(dq_z, dq_y)
    for k in range(1, nz - 1):
        pass_on(wq_z, wq_y, k)
    with jax.named_scope("wait_tp"):
        for c in tiles:
            c.wait_recv()
    tile_fs[0] = jnp.sum(tile_tp[...], axis=0)
    tiles = []
    for d in range(1, n):
        k = room(1)
        tiles.append(launch(remote(tile_fs.at[0], tile_fs.at[d], {"fs": (f + d) % n}, k, k)))
    forward_directions(do_z, do_y)
    hand(wo_y)
    hand(wq_y)
    with jax.named_scope("wait_fs"):
        for c in tiles:
            c.wait_recv()
    total[...] = jnp.sum(tile_fs[...], axis=0)
    with jax.named_scope("wait_dy"):
        for zz in [z] + others:
            do_y.wait(zz)
            dq_y.wait(zz)
    with jax.named_scope("wait_wy"):
        for c in handed:
            c.got.wait_recv()
        if mated:
            wo_z.wait(others[0])
            wq_z.wait(others[0])
        for zz in others[1:] if mated else [z] + others:
            wo_y.wait(zz)
            wq_y.wait(zz)
    with jax.named_scope("wait_send"):
        for c in sent:
            c.wait_send()
    for zz, c in low_sent:
        pl.when(zz != z)(c.wait_send)
    for free, c in far:
        pl.when(free)(c.wait_send)
    for here, c in ahead:
        pl.when(z == here)(c.wait_send)


def finish_kernel(
    nz, ny, nt,
    fq_all, fo_all, wq_all, wo_all, dq_all, do_all, total, wq, wo, qm, qs, om, os_,
    step_q_hbm, step_o_hbm, new_q_hbm, new_o_hbm, copy_q_hbm, copy_o_hbm,
    qm_hbm, qs_hbm, om_hbm, os_hbm,
    step_q, step_o, new_q, new_o, copy_q, copy_o,
    sem,
):
    f = lax.axis_index("fs")
    z, y = f // ny, f % ny
    started = []

    def put(src, dst):
        c = pltpu.make_async_copy(src, dst, sem.at[len(started)])
        c.start()
        started.append(c)

    for src, dst in ((qm, qm_hbm), (qs, qs_hbm), (om, om_hbm), (os_, os_hbm)):
        put(src, dst)
    rank = 2 * fq_all.shape[-1]
    middle = total.shape[1] // 2
    for slot, f_all, w_all, d_all, w, step, new, copy, step_hbm, new_hbm, copy_hbm in (
        (middle, fo_all, wo_all, do_all, wo, step_o, new_o, copy_o, step_o_hbm, new_o_hbm, copy_o_hbm),
        (0, fq_all, wq_all, dq_all, wq, step_q, new_q, copy_q, step_q_hbm, new_q_hbm, copy_q_hbm),
    ):
        cols = w.shape[1]
        scale = lax.rsqrt(total[...] / (rank * cols * nt) + 0.25)[:, slot:slot + 1]
        direction = d_all[...].reshape(rank, cols)
        rows = f_all.shape[3]

        def factor_rows(i, f_all=f_all):
            return jnp.concatenate([f_all[h, i].reshape(-1, rank // 2) for h in range(2)], axis=1)

        for i in range(nz):
            full = jnp.dot(
                factor_rows(i), direction, preferred_element_type=F32
            ) * scale
            at = pl.ds(i * ny * rows, ny * rows)
            old = w_all[i].reshape(ny * rows, cols).astype(F32)
            copy[at, :] = (old - 0.02 * full).astype(BF16)
            put(copy.at[at, :], copy_hbm.at[at, :])
        mine = jnp.concatenate([f_all[h, z, y] for h in range(2)], axis=1)
        own = jnp.dot(mine, direction, preferred_element_type=F32) * scale
        step[...] = own
        new[...] = w[...] - 0.02 * own
        put(step, step_hbm)
        put(new, new_hbm)
    for c in started:
        c.wait()


def on_device(
    nz, ny, nt,
    latent_in, query_cot, attn_out, mix_cot, query_weight, output_weight,
    query_factor, output_factor, query_mean, query_square, output_mean, output_square,
):
    n = nz * ny
    tokens = latent_in.shape[0]
    inv_root = 1.0 / math.sqrt(tokens * n)
    rq, cq = query_weight.shape
    ro, co = output_weight.shape
    rank = query_factor.shape[1]
    block = rank // n
    vmem = pl.BlockSpec(memory_space=pltpu.VMEM)
    hbm = pl.BlockSpec(memory_space=pltpu.HBM)
    copies = semaphores_of(nz, ny, nt)

    def exchange(*refs):
        pl.run_scoped(
            functools.partial(exchange_kernel, nz, ny, nt, inv_root, *refs),
            pltpu.SemaphoreType.DMA((CHUNKS, 4)),
            pltpu.SemaphoreType.DMA((8,)),
            pltpu.SemaphoreType.DMA((copies,)),
            pltpu.SemaphoreType.DMA((copies,)),
        )

    fq, fo, wq, wo, dq, do, total, qm, qs, om, os_ = pl.pallas_call(
        exchange,
        name="moment_exchange",
        in_specs=[hbm] * 12,
        out_specs=[vmem] * 11,
        out_shape=[
            jax.ShapeDtypeStruct((2, nz, ny, rq, rank // 2), BF16),
            jax.ShapeDtypeStruct((2, nz, ny, ro, rank // 2), BF16),
            jax.ShapeDtypeStruct((nz, ny, rq, cq), BF16),
            jax.ShapeDtypeStruct((nz, ny, ro, co), BF16),
            jax.ShapeDtypeStruct((nz, ny, block, cq), BF16),
            jax.ShapeDtypeStruct((nz, ny, block, co), BF16),
            jax.ShapeDtypeStruct((1, 128), F32),
            jax.ShapeDtypeStruct((block, cq), F32),
            jax.ShapeDtypeStruct((block, cq), F32),
            jax.ShapeDtypeStruct((block, co), F32),
            jax.ShapeDtypeStruct((block, co), F32),
        ],
        scratch_shapes=[
            pltpu.VMEM(latent_in.shape, BF16),
            pltpu.VMEM(query_cot.shape, BF16),
            pltpu.VMEM(attn_out.shape, BF16),
            pltpu.VMEM(mix_cot.shape, BF16),
            pltpu.VMEM((rq, cq), F32),
            pltpu.VMEM((ro, co), F32),
            pltpu.VMEM((block, cq), F32),
            pltpu.VMEM((block, cq), F32),
            pltpu.VMEM((block, co), F32),
            pltpu.VMEM((block, co), F32),
            pltpu.VMEM((cq, n * rq), F32),
            pltpu.VMEM((co, n * ro), F32),
            pltpu.VMEM((nz, ny, block, cq), F32),
            pltpu.VMEM((nz, ny, block, co), F32),
            pltpu.VMEM((2 * max(ny - 1, 1), nz, block, cq), BF16),
            pltpu.VMEM((2 * max(ny - 1, 1), nz, block, co), BF16),
            pltpu.VMEM((nz, block, cq), F32),
            pltpu.VMEM((nz, block, co), F32),
            pltpu.VMEM((nz, block, cq), BF16),
            pltpu.VMEM((nz, block, co), BF16),
            pltpu.VMEM((nz, block, cq), BF16),
            pltpu.VMEM((nz, block, co), BF16),
            pltpu.VMEM((nt, 1, 128), F32),
            pltpu.VMEM((n, 1, 128), F32),
            pltpu.VMEM((cq, n * rq), BF16),
            pltpu.VMEM((co, n * ro), BF16),
        ],
        compiler_params=pltpu.CompilerParams(
            collective_id=0, has_side_effects=True, vmem_limit_bytes=40 * 1024 * 1024
        ),
    )(*(pltpu.with_memory_space_constraint(a, pltpu.HBM) for a in (
        latent_in, query_cot, attn_out, mix_cot, query_weight, output_weight,
        query_factor, output_factor, query_mean, query_square, output_mean, output_square,
    )))
    shapes = (
        ((rq, cq), F32), ((ro, co), F32), ((rq, cq), F32), ((ro, co), F32),
        ((n * rq, cq), BF16), ((n * ro, co), BF16),
        ((block, cq), F32), ((block, cq), F32), ((block, co), F32), ((block, co), F32),
    )

    def finish(*refs):
        pl.run_scoped(
            functools.partial(finish_kernel, nz, ny, nt, *refs),
            pltpu.SemaphoreType.DMA((2 * nz + 8,)),
        )

    return pl.pallas_call(
        finish,
        name="finish",
        in_specs=[vmem] * 13,
        out_specs=[hbm] * 10,
        out_shape=[jax.ShapeDtypeStruct(*s) for s in shapes],
        scratch_shapes=[pltpu.VMEM(*s) for s in shapes[:6]],
        compiler_params=pltpu.CompilerParams(vmem_limit_bytes=20 * 1024 * 1024),
    )(fq, fo, wq, wo, dq, do, total, query_weight, output_weight, qm, qs, om, os_)


def solution(mesh):
    nz, ny = grid_of(mesh.shape["fs"])
    rows, both, cols = P("fs", None), P("fs", "tp"), P(None, "tp")
    return jax.shard_map(
        functools.partial(on_device, nz, ny, mesh.shape["tp"]),
        mesh=mesh,
        in_specs=(rows, both, rows, both, both, both, rows, rows, both, both, both, both),
        out_specs=(both, both, both, both, cols, cols, both, both, both, both),
        check_vma=False,
    )
```

```python
import functools
import math

import jax
import jax.numpy as jnp
from jax import lax
from jax.experimental import pallas as pl
from jax.experimental.pallas import tpu as pltpu
from jax.sharding import PartitionSpec as P

MESH = pl.DeviceIdType.MESH
BF16 = jnp.bfloat16
F32 = jnp.float32
CHUNKS = 4


def grid_of(count):
    inner = max(d for d in range(1, count + 1) if count % d == 0 and d * d <= count)
    return count // inner, inner


def semaphores_of(nz, ny, nt):
    z_kinds, y_kinds = 2 + 2 + 2 + 2, 2 + 2 + 2
    return z_kinds * nz + y_kinds * nz * (ny - 1) + 6 * (ny - 1) + 2 * ny + nt + nz * ny + 4 + ny * nt


def over_rows(left, right):
    return lax.dot_general(left, right, (((0,), (0,)), ((), ())), preferred_element_type=F32)


def exchange_kernel(
    nz, ny, nt, inv_root,
    latent_hbm, cot_hbm, attn_hbm, mix_hbm, wq_hbm, wo_hbm, fq_hbm, fo_hbm,
    qm_hbm, qs_hbm, om_hbm, os_hbm,
    fq_all, fo_all, wq_all, wo_all, dq_all, do_all, total, qm_new, qs_new, om_new, os_new,
    latent, cot, attn, mix, wq, wo, qm, qs, om, os_, grad_q, grad_o,
    part_q, part_o, yin_q, yin_o, acc_q, acc_o, zout_q, zout_o, zin_q, zin_o,
    tile_tp, tile_fs, rounded_q, rounded_o,
    load_sem, own_sem, send_sem, recv_sem,
):
    n = nz * ny
    f = lax.axis_index("fs")
    t = lax.axis_index("tp")
    z, y = f // ny, f % ny
    half_cols = fq_all.shape[-1]
    core = t % 2
    half = pl.ds(pl.multiple_of(core * half_cols, half_cols), half_cols)
    twin = t + 1 - 2 * (t % 2)
    step = latent_hbm.shape[0] // CHUNKS
    shares = nt // 2 if fo_hbm.shape[0] % (16 * (nt // 2)) == 0 else 1
    share_rows = fo_hbm.shape[0] // shares
    share = pl.ds(pl.multiple_of((t // 2) % shares * share_rows, share_rows), share_rows)

    barrier = pltpu.get_barrier_semaphore()
    for d in range(1, n):
        pl.semaphore_signal(barrier, inc=1, device_id={"fs": (f + d) % n}, device_id_type=MESH)
    for d in range(1, nt):
        pl.semaphore_signal(barrier, inc=1, device_id={"tp": (t + d) % nt}, device_id_type=MESH)

    own = [
        pltpu.make_async_copy(src, dst, own_sem.at[i])
        for i, (src, dst) in enumerate((
            (fo_hbm.at[share, half], fo_all.at[core, z, y, share]),
            (fq_hbm.at[:, half], fq_all.at[core, z, y]),
            (wo_hbm, wo), (wq_hbm, wq),
            (om_hbm, om), (os_hbm, os_), (qm_hbm, qm), (qs_hbm, qs),
        ))
    ]
    for c in own[:4]:
        c.start()

    def load(k, pair, sem):
        rows = pl.ds(pl.multiple_of(k * step, step), step)
        return [
            pltpu.make_async_copy(src.at[rows, :], dst.at[rows, :], load_sem.at[k, sem + i])
            for i, (src, dst) in enumerate(pair)
        ]

    pair_o = ((attn_hbm, attn), (mix_hbm, mix))
    pair_q = ((latent_hbm, latent), (cot_hbm, cot))
    with jax.named_scope("own"):
        for c in own[:4]:
            c.wait()
    for k in range(CHUNKS):
        for c in load(k, pair_q, 2):
            c.start()
    for k in range(CHUNKS):
        for c in load(k, pair_o, 0):
            c.start()
    for c in own[4:]:
        c.start()
    wo_all[z, y] = wo[...].astype(BF16)
    wq_all[z, y] = wq[...].astype(BF16)
    with jax.named_scope("barrier"):
        pl.semaphore_wait(barrier, n - 1 + nt - 1)

    used = [0]
    sent = []

    def room(count):
        at = used[0]
        used[0] = at + count
        return at

    def remote(src, dst, device, at, to):
        return pltpu.make_async_remote_copy(
            src_ref=src, dst_ref=dst, send_sem=send_sem.at[at], recv_sem=recv_sem.at[to],
            device_id=device, device_id_type=MESH,
        )

    def launch(c):
        c.start()
        sent.append(c)
        return c

    lower, upper = z, nz - 1 - z
    both = jnp.minimum(lower, upper)

    def near(k):
        paired = k < 2 * both
        away = jnp.where(paired, k // 2 + 1, k - both + 1)
        down = jnp.where(paired, (k + z) % 2 == 1, lower > upper)
        return jnp.where(down, z - away, z + away)

    others = [near(k) for k in range(nz - 1)]

    class Along:
        def __init__(self, block, landing=None):
            self.block, self.landing, self.at = block, landing or block, room(nz)

        def to(self, zz):
            return remote(
                self.block(z) if self.landing is self.block else self.block(zz), self.landing(z),
                {"fs": zz * ny + y}, self.at + zz, self.at + z,
            )

        def wait(self, zz):
            remote(
                self.landing(zz), self.landing(zz), {"fs": zz * ny + y}, self.at + zz, self.at + zz
            ).wait_recv()

    class Across:
        def __init__(self, block):
            self.block, self.at = block, room(nz * (ny - 1))

        def copies(self, zz):
            ks = [self.at + (d - 1) * nz + zz for d in range(1, ny)]
            return [
                remote(self.block(zz, y), self.block(zz, y), {"fs": z * ny + (y + d) % ny}, k, k)
                for d, k in zip(range(1, ny), ks)
            ]

        def send(self, zz):
            for c in self.copies(zz):
                launch(c)

        def wait(self, zz):
            for d in range(1, ny):
                k = self.at + (d - 1) * nz + zz
                block = self.block(zz, (y + ny - d) % ny)
                remote(block, block, {"fs": z * ny + (y + d) % ny}, k, k).wait_recv()

    fo_z = Along(lambda zz: fo_all.at[core, zz, y, share])
    fq_z = Along(lambda zz: fq_all.at[core, zz, y])
    fo_y = Across(lambda zz, yy: fo_all.at[core, zz, yy, share])
    fq_y = Across(lambda zz, yy: fq_all.at[core, zz, yy])
    wo_z = Along(lambda zz: wo_all.at[zz, y])
    wq_z = Along(lambda zz: wq_all.at[zz, y])
    wo_y = Across(lambda zz, yy: wo_all.at[zz, yy])
    wq_y = Across(lambda zz, yy: wq_all.at[zz, yy])
    do_z = Along(lambda zz: do_all.at[zz, y])
    dq_z = Along(lambda zz: dq_all.at[zz, y])
    do_y = Across(lambda zz, yy: do_all.at[zz, yy])
    dq_y = Across(lambda zz, yy: dq_all.at[zz, yy])

    for fac_z, fac_y in ((fq_z, fq_y), (fo_z, fo_y)):
        for zz in others:
            launch(fac_z.to(zz))
        fac_y.send(z)
    wo_y.send(z)

    through = nz >= 3
    mated = nz % 2 == 0
    inside = jnp.logical_and(z > 0, z < nz - 1)
    far = []

    def send_weights(w_z):
        for k, zz in enumerate(others):
            c = w_z.to(zz)
            if through and k > 0:
                free = jnp.logical_or(
                    jnp.logical_and(zz > 0, zz < nz - 1), jnp.logical_or(zz == z + 1, zz == z - 1)
                )
                far.append((free, c))
                pl.when(free)(c.start)
            else:
                launch(c)

    def product(k, pair, sem, out):
        for c in load(k, pair, sem):
            c.wait()
        rows = pl.ds(pl.multiple_of(k * step, step), step)
        new = over_rows(pair[1][1][rows, :], pair[0][1][rows, :])
        out[...] += new

    def products(lo, hi, pair, sem, out):
        @pl.loop(lo, hi)
        def _(k):
            product(k, pair, sem, out)

    grad_o[...] = jnp.zeros_like(grad_o)
    grad_q[...] = jnp.zeros_like(grad_q)
    swaps = {}

    def swap(all_, yy):
        block = all_.at[core, :, yy]
        k = room(1)
        return launch(remote(block, block, {"tp": twin}, k, k))

    def to_chips(yy):
        out = []
        for d in range(1, shares):
            block = fo_all.at[core, :, yy, share]
            k = room(1)
            out.append(launch(remote(block, block, {"tp": (t + 2 * d) % nt}, k, k)))
        return out

    def arrived(copies):
        with jax.named_scope("wait_x"):
            for c in copies:
                c.wait_recv()

    done = 0

    def more_o(upto):
        nonlocal done
        if done < upto:
            with jax.named_scope("prod_o"):
                products(done, upto, pair_o, 0, grad_o)
            done = upto

    with jax.named_scope("prod_q"):
        products(0, CHUNKS, pair_q, 2, grad_q)
    more_o(1)
    for zz in others:
        with jax.named_scope("wait_fqz"):
            fq_z.wait(zz)
        fq_y.send(zz)
    swaps["q"] = [swap(fq_all, y)]
    send_weights(wo_z)
    send_weights(wq_z)
    for k, zz in enumerate(others):
        with jax.named_scope("wait_foz"):
            fo_z.wait(zz)
        fo_y.send(zz)
    near_o = to_chips(y)
    more_o(CHUNKS - 1)
    across_o = []

    rank = 2 * half_cols
    block = rank // n
    per_half = nz // 2

    def project(h, factor_all, grad, part):
        factor = factor_all[h].reshape(-1, half_cols)
        low = lax.dot_general(
            factor, grad[...], (((0,), (1,)), ((), ())), preferred_element_type=F32
        ) * inv_root
        for i in range(per_half):
            for j in range(ny):
                at = (i * ny + j) * block
                part[h * per_half + i, j] = low[at:at + block, :]

    matrices = (
        ("q", fq_all, fq_y, grad_q, rounded_q, part_q, yin_q, acc_q, zout_q, zin_q),
        ("o", fo_all, fo_y, grad_o, rounded_o, part_o, yin_o, acc_o, zout_o, zin_o),
    )
    ahead = []

    def relay(w_z, ks):
        for k in ks if through else ():
            mine = []
            for edge, here in ((0, 1), (nz - 1, nz - 2)):
                at = room(1)
                mine.append((here, remote(
                    w_z.block(others[k]), w_z.block(others[k]), {"fs": edge * ny + y},
                    at, w_z.at + others[k],
                )))
            with jax.named_scope("wait_far"):
                pl.when(inside)(lambda: w_z.wait(others[k]))
            for here, c in mine:
                pl.when(z == here)(c.start)
            ahead.extend(mine)

    def pass_on(w_z, w_y, k):
        with jax.named_scope("wait_edge"):
            if through:
                pl.when(jnp.logical_not(inside))(lambda: w_z.wait(others[k]))
            else:
                w_z.wait(others[k])
        w_y.send(others[k])

    units = []
    for name, all_, fac_y, grad, rounded, part, yin, acc, zout, zin in matrices:
        if name == "o":
            wq_y.send(z)
            more_o(CHUNKS)
            arrived(across_o)
        rounded[...] = grad[...].astype(BF16)
        along = Along(lambda zz, zout=zout: zout.at[zz], lambda zz, zin=zin: zin.at[zz])
        if name == "q":
            with jax.named_scope("wait_fy"):
                for zz in [z] + others:
                    fac_y.wait(zz)
        for d in range(1, ny):
            swaps[name].append(swap(all_, (y + ny - d) % ny))
        for turn, h in enumerate((core, 1 - core)):
            if turn and name == "q":
                with jax.named_scope("wait_foy"):
                    for zz in [z] + others:
                        fo_y.wait(zz)
                for d in range(1, ny):
                    across_o += to_chips((y + ny - d) % ny)
                arrived(near_o)
                swaps["o"] = [swap(fo_all, y)]
            if turn:
                with jax.named_scope("wait_swap"):
                    for c in swaps[name]:
                        c.wait_recv()
            with jax.named_scope("project"):
                project(h, all_, rounded, part)
            rows = pl.ds(h * per_half, per_half)
            copies = []
            for d in range(1, ny):
                yy = (y + d) % ny
                for i in range(per_half):
                    yin[ny - 1 + d - 1, h * per_half + i] = part[h * per_half + i, yy].astype(BF16)
                k = room(1)
                copies.append(launch(remote(
                    yin.at[ny - 1 + d - 1, rows], yin.at[d - 1, rows], {"fs": z * ny + yy}, k, k
                )))
            if name == "q" and turn == 1:
                relay(wo_z, range(1, min(2, nz - 1)))
            if name == "o" and turn == 0:
                relay(wo_z, range(2, nz - 1))
            units.append((h, part, yin, acc, zout, along, copies))

    def forward(k, w_z, w_y):
        with jax.named_scope("wait_wz"):
            w_z.wait(others[k])
        w_y.send(others[k])

    if nz > 1 and not mated:
        forward(0, wo_z, wo_y)
        forward(0, wq_z, wq_y)

    def hand_over(w_y):
        mate = z + 1 - 2 * (z % 2)
        out = []
        for d in range(1, ny):
            yy = (y + d) % ny
            k = room(1)
            out.append(remote(w_y.block(z, yy), w_y.block(z, yy), {"fs": mate * ny + y}, k, k))
            out[-1].got = remote(
                w_y.block(mate, yy), w_y.block(mate, yy), {"fs": mate * ny + y}, k, k
            )
        return out

    low_sent = []
    for turn, (h, part, yin, acc, zout, along, copies) in enumerate(units):
        if turn == 3:
            relay(wq_z, range(1, nz - 1))
        if turn == 3 and nz > 2:
            pass_on(wo_z, wo_y, 1)
        for i in range(per_half):
            acc[h * per_half + i] = part[h * per_half + i, y]
        for d, c in enumerate(copies):
            with jax.named_scope("wait_y"):
                c.wait_recv()
            for i in range(per_half):
                acc[h * per_half + i] += yin[d, h * per_half + i].astype(F32)
        for i in range(per_half):
            zz = h * per_half + i
            zout[zz] = acc[zz].astype(BF16)
            c = along.to(zz)
            pl.when(zz != z)(c.start)
            low_sent.append((zz, c))

    sides = (
        (matrices[0], units[0][5], qm, qs, qm_new, qs_new, dq_all, dq_z, dq_y),
        (matrices[1], units[2][5], om, os_, om_new, os_new, do_all, do_z, do_y),
    )
    for c in own[4:]:
        c.wait()
    squares = []
    for matrix, along, mean, square, mean_out, square_out, d_all, d_z, d_y in sides:
        acc, zin = matrix[7], matrix[9]
        low = acc[z]
        for zz in others:
            with jax.named_scope("wait_z"):
                along.wait(zz)
            low += zin[zz].astype(F32)
        mean_new = 0.8 * mean[...] + 0.2 * low
        square_new = 0.9 * square[...] + 0.1 * low * low
        mean_out[...] = mean_new
        square_out[...] = square_new
        direction = mean_new / jnp.sqrt(square_new)
        d_all[z, y] = direction.astype(BF16)
        for zz in others:
            launch(d_z.to(zz))
        d_y.send(z)
        squares.append(jnp.sum(direction * direction))
        if len(squares) == 1:
            for k in range(2, nz - 1):
                pass_on(wo_z, wo_y, k)
    lanes = lax.broadcasted_iota(jnp.int32, tile_tp.shape[1:], 1)
    tile_tp[0] = jnp.where(lanes < tile_tp.shape[2] // 2, squares[0], squares[1])

    tiles = []
    for d in range(1, nt):
        k = room(1)
        tiles.append(launch(remote(tile_tp.at[0], tile_tp.at[d], {"tp": (t + d) % nt}, k, k)))

    def forward_directions(d_z, d_y, ks):
        for zz in [others[k] for k in ks]:
            with jax.named_scope("wait_dz"):
                d_z.wait(zz)
            d_y.send(zz)

    handed = []

    def hand(w_y):
        if mated:
            w_y.wait(z)
            for c in hand_over(w_y):
                handed.append(launch(c))

    forward_directions(dq_z, dq_y, range(nz - 1))
    for k in range(1, nz - 1):
        pass_on(wq_z, wq_y, k)
    forward_directions(do_z, do_y, range(min(1, nz - 1)))
    with jax.named_scope("wait_tp"):
        for c in tiles:
            c.wait_recv()
    tile_fs[0] = jnp.sum(tile_tp[...], axis=0)
    tiles = []
    for d in range(1, n):
        k = room(1)
        tiles.append(launch(remote(tile_fs.at[0], tile_fs.at[d], {"fs": (f + d) % n}, k, k)))
    hand(wo_y)
    hand(wq_y)
    forward_directions(do_z, do_y, range(1, nz - 1))
    with jax.named_scope("wait_fs"):
        for c in tiles:
            c.wait_recv()
    total[...] = jnp.sum(tile_fs[...], axis=0)
    with jax.named_scope("wait_dy"):
        for zz in [z] + others:
            do_y.wait(zz)
            dq_y.wait(zz)
    with jax.named_scope("wait_wy"):
        for c in handed:
            c.got.wait_recv()
        if mated:
            wo_z.wait(others[0])
            wq_z.wait(others[0])
        for zz in others[1:] if mated else [z] + others:
            wo_y.wait(zz)
            wq_y.wait(zz)
    with jax.named_scope("wait_send"):
        for c in sent:
            c.wait_send()
    for zz, c in low_sent:
        pl.when(zz != z)(c.wait_send)
    for free, c in far:
        pl.when(free)(c.wait_send)
    for here, c in ahead:
        pl.when(z == here)(c.wait_send)


def finish_kernel(
    nz, ny, nt,
    fq_all, fo_all, wq_all, wo_all, dq_all, do_all, total, wq, wo, qm, qs, om, os_,
    step_q_hbm, step_o_hbm, new_q_hbm, new_o_hbm, copy_q_hbm, copy_o_hbm,
    qm_hbm, qs_hbm, om_hbm, os_hbm,
    step_q, step_o, new_q, new_o, copy_q, copy_o,
    sem,
):
    f = lax.axis_index("fs")
    z, y = f // ny, f % ny
    started = []

    def put(src, dst):
        c = pltpu.make_async_copy(src, dst, sem.at[len(started)])
        c.start()
        started.append(c)

    for src, dst in ((qm, qm_hbm), (qs, qs_hbm), (om, om_hbm), (os_, os_hbm)):
        put(src, dst)
    rank = 2 * fq_all.shape[-1]
    middle = total.shape[1] // 2
    for slot, f_all, w_all, d_all, w, step, new, copy, step_hbm, new_hbm, copy_hbm in (
        (middle, fo_all, wo_all, do_all, wo, step_o, new_o, copy_o, step_o_hbm, new_o_hbm, copy_o_hbm),
        (0, fq_all, wq_all, dq_all, wq, step_q, new_q, copy_q, step_q_hbm, new_q_hbm, copy_q_hbm),
    ):
        cols = w.shape[1]
        scale = lax.rsqrt(total[...] / (rank * cols * nt) + 0.25)[:, slot:slot + 1]
        direction = d_all[...].reshape(rank, cols)
        rows = f_all.shape[3]

        def factor_rows(i, f_all=f_all):
            return jnp.concatenate([f_all[h, i].reshape(-1, rank // 2) for h in range(2)], axis=1)

        for i in range(nz):
            full = jnp.dot(
                factor_rows(i), direction, preferred_element_type=F32
            ) * scale
            at = pl.ds(i * ny * rows, ny * rows)
            old = w_all[i].reshape(ny * rows, cols).astype(F32)
            copy[at, :] = (old - 0.02 * full).astype(BF16)
            put(copy.at[at, :], copy_hbm.at[at, :])
        mine = jnp.concatenate([f_all[h, z, y] for h in range(2)], axis=1)
        own = jnp.dot(mine, direction, preferred_element_type=F32) * scale
        step[...] = own
        new[...] = w[...] - 0.02 * own
        put(step, step_hbm)
        put(new, new_hbm)
    for c in started:
        c.wait()


def on_device(
    nz, ny, nt,
    latent_in, query_cot, attn_out, mix_cot, query_weight, output_weight,
    query_factor, output_factor, query_mean, query_square, output_mean, output_square,
):
    n = nz * ny
    tokens = latent_in.shape[0]
    inv_root = 1.0 / math.sqrt(tokens * n)
    rq, cq = query_weight.shape
    ro, co = output_weight.shape
    rank = query_factor.shape[1]
    block = rank // n
    vmem = pl.BlockSpec(memory_space=pltpu.VMEM)
    hbm = pl.BlockSpec(memory_space=pltpu.HBM)
    copies = semaphores_of(nz, ny, nt)

    def exchange(*refs):
        pl.run_scoped(
            functools.partial(exchange_kernel, nz, ny, nt, inv_root, *refs),
            pltpu.SemaphoreType.DMA((CHUNKS, 4)),
            pltpu.SemaphoreType.DMA((8,)),
            pltpu.SemaphoreType.DMA((copies,)),
            pltpu.SemaphoreType.DMA((copies,)),
        )

    fq, fo, wq, wo, dq, do, total, qm, qs, om, os_ = pl.pallas_call(
        exchange,
        name="moment_exchange",
        in_specs=[hbm] * 12,
        out_specs=[vmem] * 11,
        out_shape=[
            jax.ShapeDtypeStruct((2, nz, ny, rq, rank // 2), BF16),
            jax.ShapeDtypeStruct((2, nz, ny, ro, rank // 2), BF16),
            jax.ShapeDtypeStruct((nz, ny, rq, cq), BF16),
            jax.ShapeDtypeStruct((nz, ny, ro, co), BF16),
            jax.ShapeDtypeStruct((nz, ny, block, cq), BF16),
            jax.ShapeDtypeStruct((nz, ny, block, co), BF16),
            jax.ShapeDtypeStruct((1, 128), F32),
            jax.ShapeDtypeStruct((block, cq), F32),
            jax.ShapeDtypeStruct((block, cq), F32),
            jax.ShapeDtypeStruct((block, co), F32),
            jax.ShapeDtypeStruct((block, co), F32),
        ],
        scratch_shapes=[
            pltpu.VMEM(latent_in.shape, BF16),
            pltpu.VMEM(query_cot.shape, BF16),
            pltpu.VMEM(attn_out.shape, BF16),
            pltpu.VMEM(mix_cot.shape, BF16),
            pltpu.VMEM((rq, cq), F32),
            pltpu.VMEM((ro, co), F32),
            pltpu.VMEM((block, cq), F32),
            pltpu.VMEM((block, cq), F32),
            pltpu.VMEM((block, co), F32),
            pltpu.VMEM((block, co), F32),
            pltpu.VMEM((cq, n * rq), F32),
            pltpu.VMEM((co, n * ro), F32),
            pltpu.VMEM((nz, ny, block, cq), F32),
            pltpu.VMEM((nz, ny, block, co), F32),
            pltpu.VMEM((2 * max(ny - 1, 1), nz, block, cq), BF16),
            pltpu.VMEM((2 * max(ny - 1, 1), nz, block, co), BF16),
            pltpu.VMEM((nz, block, cq), F32),
            pltpu.VMEM((nz, block, co), F32),
            pltpu.VMEM((nz, block, cq), BF16),
            pltpu.VMEM((nz, block, co), BF16),
            pltpu.VMEM((nz, block, cq), BF16),
            pltpu.VMEM((nz, block, co), BF16),
            pltpu.VMEM((nt, 1, 128), F32),
            pltpu.VMEM((n, 1, 128), F32),
            pltpu.VMEM((cq, n * rq), BF16),
            pltpu.VMEM((co, n * ro), BF16),
        ],
        compiler_params=pltpu.CompilerParams(
            collective_id=0, has_side_effects=True, vmem_limit_bytes=40 * 1024 * 1024
        ),
    )(*(pltpu.with_memory_space_constraint(a, pltpu.HBM) for a in (
        latent_in, query_cot, attn_out, mix_cot, query_weight, output_weight,
        query_factor, output_factor, query_mean, query_square, output_mean, output_square,
    )))
    shapes = (
        ((rq, cq), F32), ((ro, co), F32), ((rq, cq), F32), ((ro, co), F32),
        ((n * rq, cq), BF16), ((n * ro, co), BF16),
        ((block, cq), F32), ((block, cq), F32), ((block, co), F32), ((block, co), F32),
    )

    def finish(*refs):
        pl.run_scoped(
            functools.partial(finish_kernel, nz, ny, nt, *refs),
            pltpu.SemaphoreType.DMA((2 * nz + 8,)),
        )

    return pl.pallas_call(
        finish,
        name="finish",
        in_specs=[vmem] * 13,
        out_specs=[hbm] * 10,
        out_shape=[jax.ShapeDtypeStruct(*s) for s in shapes],
        scratch_shapes=[pltpu.VMEM(*s) for s in shapes[:6]],
        compiler_params=pltpu.CompilerParams(vmem_limit_bytes=20 * 1024 * 1024),
    )(fq, fo, wq, wo, dq, do, total, query_weight, output_weight, qm, qs, om, os_)


def solution(mesh):
    nz, ny = grid_of(mesh.shape["fs"])
    rows, both, cols = P("fs", None), P("fs", "tp"), P(None, "tp")
    return jax.shard_map(
        functools.partial(on_device, nz, ny, mesh.shape["tp"]),
        mesh=mesh,
        in_specs=(rows, both, rows, both, both, both, rows, rows, both, both, both, both),
        out_specs=(both, both, both, both, cols, cols, both, both, both, both),
        check_vma=False,
    )
```
